32 devices in a mesh: ep: 32 (over z, y, x, core).
Axes of the slice: x: 2, y: 2, z: 4, core: 2. Of those that a mesh axis runs over, the one named last changes fastest.
Arguments:
- tokens: bfloat16 [768, 2048], P('ep'), may hold values from -6 to 6
- state: float32 [768, 16, 64, 64], P('ep'), may hold values from -4 to 4
- norm_gain: float32 [2048], replicated, may hold values from 0.1 to 1.9
- w_recept: bfloat16 [2048, 1024], replicated, may hold values from -0.125 to 0.125
- w_keys: bfloat16 [2048, 1024], replicated, may hold values from -0.125 to 0.125
- w_values: bfloat16 [2048, 1024], replicated, may hold values from -0.125 to 0.125
- decay_base: float32 [1024], replicated, may hold values from -3 to 3
- decay_first_matrix: bfloat16 [2048, 128], replicated, may hold values from -0.125 to 0.125
- decay_second_matrix: bfloat16 [128, 1024], replicated, may hold values from -0.5 to 0.5
- rate_base: float32 [1024], replicated, may hold values from -3 to 3
- rate_first_matrix: bfloat16 [2048, 128], replicated, may hold values from -0.125 to 0.125
- rate_second_matrix: bfloat16 [128, 1024], replicated, may hold values from -0.5 to 0.5
- head_gain: float32 [1024], replicated, may hold values from 0.1 to 1.9
- w_output: bfloat16 [1024, 2048], replicated, may hold values from -0.1875 to 0.1875
- second_gain: float32 [2048], replicated, may hold values from 0.1 to 1.9
- route_ids: int32 [768, 2], replicated, may hold values from 0 to 15, all different within a row; in each aligned block of 24 rows (0 to 23, 24 to 47, ...) at most 6 rows name the same one
- route_weights: float32 [768, 2], replicated, may hold values from 0.2 to 1
- expert_gate: bfloat16 [2048, 49152], P(None, 'ep'), may hold values from -0.125 to 0.125
- expert_up: bfloat16 [2048, 49152], P(None, 'ep'), may hold values from -0.125 to 0.125
- expert_down: bfloat16 [49152, 2048], P('ep'), may hold values from -0.109375 to 0.109375
Outputs:
- layer_out: bfloat16 [768, 2048], P('ep')
- new_state: float32 [768, 16, 64, 64], P('ep')
The draws below stay inside these ranges and needn't reach their ends.
Inputs may be any that keep to these rules, and one draw needn't show every extreme that they name: `route_ids`: each row names 2 different experts. Among the 24 rows of one device (aligned blocks), no expert is named by more than 6 rows, and in every draw some block names some expert exactly 6 times.
All inputs are finite; a program needn't handle non-finite values.
Results may differ from the reference program's by a relative error of at most 0.015.
Values may be sent and summed in bfloat16 or wider, within the bound.
No kernel may reach another device: no remote copies, remote signals or barrier semaphores. Data moves between devices by JAX's collectives and lax.ppermute only.
A program may use at most 192 MiB of HBM per device.

```python
import math
import jax
import jax.numpy as jnp
import numpy as np
from jax import lax

MODEL_WIDTH = 2048
MIXER_HEADS = 16
HEAD_SIZE = 64
LOWRANK_WIDTH = 128
EXPERTS = 16
FF_E = 3072
TOPK = 2
SEQ_DEV = 24
CAP_DEV = 6
BATCH = 768
N_EP = 32


def levels(stream_key, dims, cuts, least, high):
    def one(axis_at, shards_of):
        heights = jax.random.uniform(jax.random.fold_in(jax.random.fold_in(stream_key, 6), axis_at), (shards_of,), jnp.float32, least / len(cuts), high / len(cuts))
        return jnp.repeat(jnp.exp(heights), dims[axis_at] // shards_of).reshape((-1,) + (1,) * (len(dims) - axis_at - 1))

    level = one(*cuts[0])
    for cut in cuts[1:]:
        level = level * one(*cut)
    return level


def assign_block(key, own, number, rows, amount, top, most, slope):
    order = jax.random.permutation(key, amount)
    heavy_load, usual = portions_of(amount, rows * top, most, slope, True), portions_of(amount, rows * top, most, slope, False)
    places = jnp.arange(amount)

    def named(lengths, turn):
        used = int((lengths > 0).sum())
        fixed = max(1, used // 4)
        moved = fixed + (places - fixed + turn * (used - fixed)) % max(1, amount - fixed)
        return jnp.zeros((amount,), jnp.int32).at[order[jnp.where(places < fixed, places, moved)]].set(jnp.asarray(lengths, jnp.int32))

    lengths = jnp.where(number % 4 == 0, named(heavy_load, number // 4), named(usual, number - number // 4 - 1))
    mixed = jax.random.permutation(jax.random.fold_in(own, 3), amount)
    donor, taker = mixed[0:amount // 2 * 2:2], mixed[1:amount // 2 * 2:2]
    room = jnp.minimum(lengths[donor] - 1, most - lengths[taker]) // 2
    room = jnp.where((donor == order[0]) | (taker == order[0]) | (lengths[taker] == 0), 0, jnp.maximum(room, 0))
    moved = jax.random.randint(jax.random.fold_in(own, 4), (amount // 2,), 0, 1 << 20) % (room + 1)
    lengths = lengths.at[donor].add(-moved).at[taker].add(moved)
    items = jnp.searchsorted(jnp.cumsum(lengths), jnp.arange(rows * top), side="right").astype(jnp.int32)
    table = items.reshape(top, rows).T
    table = table[jax.random.permutation(jax.random.fold_in(own, 1), rows)]
    turn = jax.random.randint(jax.random.fold_in(own, 2), (rows, 1), 0, top)
    return jnp.take_along_axis(table, (jnp.arange(top)[None, :] + turn) % top, axis=1)


def portions_of(number_of, total, most, slope, full):
    loads = [(1 << 20) // math.isqrt(grade ** slope) + 1 for grade in range(1, number_of + 1)]
    largest = most if full else min(most, max(-(-total // number_of), total * loads[0] // sum(loads)))
    least = 1 if total - largest >= number_of - 1 else 0
    counts, rest = [largest] + [least] * (number_of - 1), total - largest - least * (number_of - 1)
    while rest > 0:
        free = [i for i in range(1, number_of) if counts[i] < largest] or [i for i in range(1, number_of) if counts[i] < most]
        pool, left = sum([loads[i] for i in free]), rest
        for i in free:
            addition = min(most - counts[i], max(1, left * loads[i] // pool), rest)
            counts[i] = counts[i] + addition
            rest = rest - addition
    return np.array(counts)


def normal_values(stream_key, dims, scale, bound, cuts=(), held_as=jnp.bfloat16):
    level = levels(stream_key, dims, cuts, -0.22, 0.18) if cuts else 1.0
    values = jax.random.normal(stream_key, dims, jnp.float32) * scale * level
    return jnp.minimum(jnp.maximum(values, -bound), bound).astype(held_as)


def setup_inputs(seed: int = 0) -> dict:
    key_list = jax.random.split(jax.random.key(seed), 21)
    tokens = normal_values(key_list[0], (BATCH, MODEL_WIDTH), 1.0, 6.0, ((0, 32),))
    state = normal_values(key_list[1], (BATCH, MIXER_HEADS, HEAD_SIZE, HEAD_SIZE), 0.5, 4.0, ((0, 32),), jnp.float32)
    norm_gain = jnp.clip(1.0 + 0.18 * jax.random.normal(key_list[2], (MODEL_WIDTH,), jnp.float32), 0.1, 1.9)
    w_recept = normal_values(key_list[3], (MODEL_WIDTH, MIXER_HEADS * HEAD_SIZE), MODEL_WIDTH ** -0.5, 0.125)
    w_keys = normal_values(key_list[4], (MODEL_WIDTH, MIXER_HEADS * HEAD_SIZE), MODEL_WIDTH ** -0.5, 0.125)
    w_values = normal_values(key_list[5], (MODEL_WIDTH, MIXER_HEADS * HEAD_SIZE), MODEL_WIDTH ** -0.5, 0.125)
    decay_base = normal_values(key_list[6], (MIXER_HEADS * HEAD_SIZE,), 1.0, 3.0, (), jnp.float32)
    decay_first_matrix = normal_values(key_list[7], (MODEL_WIDTH, LOWRANK_WIDTH), MODEL_WIDTH ** -0.5, 0.125)
    decay_second_matrix = normal_values(key_list[8], (LOWRANK_WIDTH, MIXER_HEADS * HEAD_SIZE), LOWRANK_WIDTH ** -0.5, 0.5)
    rate_base = normal_values(key_list[9], (MIXER_HEADS * HEAD_SIZE,), 1.0, 3.0, (), jnp.float32)
    rate_first_matrix = normal_values(key_list[10], (MODEL_WIDTH, LOWRANK_WIDTH), MODEL_WIDTH ** -0.5, 0.125)
    rate_second_matrix = normal_values(key_list[11], (LOWRANK_WIDTH, MIXER_HEADS * HEAD_SIZE), LOWRANK_WIDTH ** -0.5, 0.5)
    head_gain = jnp.clip(1.0 + 0.18 * jax.random.normal(key_list[12], (MIXER_HEADS * HEAD_SIZE,), jnp.float32), 0.1, 1.9)
    w_output = normal_values(key_list[13], (MIXER_HEADS * HEAD_SIZE, MODEL_WIDTH), (MIXER_HEADS * HEAD_SIZE) ** -0.5, 0.1875)
    second_gain = jnp.clip(1.0 + 0.18 * jax.random.normal(key_list[14], (MODEL_WIDTH,), jnp.float32), 0.1, 1.9)
    route_ids_keys = jax.random.split(jax.random.fold_in(key_list[15], 1), BATCH // SEQ_DEV)
    route_ids_turns = jax.random.permutation(jax.random.fold_in(key_list[15], 3), BATCH // SEQ_DEV)
    route_ids = jax.vmap(lambda own, number: assign_block(jax.random.fold_in(key_list[15], 2), own, number, SEQ_DEV, EXPERTS, TOPK, CAP_DEV, 2))(route_ids_keys, route_ids_turns).reshape((BATCH, TOPK))
    route_weights = jnp.clip(jax.random.uniform(key_list[16], (BATCH, TOPK), jnp.float32, 0.2, 1.0), 0.2, 1.0)
    expert_gate = normal_values(key_list[17], (MODEL_WIDTH, EXPERTS * FF_E), MODEL_WIDTH ** -0.5, 0.125, ((1, 32),))
    expert_up = normal_values(key_list[18], (MODEL_WIDTH, EXPERTS * FF_E), MODEL_WIDTH ** -0.5, 0.125, ((1, 32),))
    expert_down = normal_values(key_list[19], (EXPERTS * FF_E, MODEL_WIDTH), FF_E ** -0.5, 0.109375, ((0, 32),))
    return {"tokens": tokens, "state": state, "norm_gain": norm_gain, "w_recept": w_recept, "w_keys": w_keys, "w_values": w_values, "decay_base": decay_base, "decay_first_matrix": decay_first_matrix, "decay_second_matrix": decay_second_matrix, "rate_base": rate_base, "rate_first_matrix": rate_first_matrix, "rate_second_matrix": rate_second_matrix, "head_gain": head_gain, "w_output": w_output, "second_gain": second_gain, "route_ids": route_ids, "route_weights": route_weights, "expert_gate": expert_gate, "expert_up": expert_up, "expert_down": expert_down}


def norm_rows(values, gain):
    mean_sq = lax.optimization_barrier(jnp.mean(values * values, axis=-1, keepdims=True))
    return values * lax.rsqrt(mean_sq + 1e-06) * gain

def time_mixer(tokens, state, norm_gain, w_recept, w_keys, w_values, decay_base, decay_first_matrix, decay_second_matrix, rate_base, rate_first_matrix, rate_second_matrix, head_gain, w_output):
    count = tokens.shape[0]
    heads = state.shape[1]
    width = state.shape[2]
    resid = tokens.astype(jnp.float32)
    normed = norm_rows(resid, norm_gain).astype(jnp.bfloat16)
    recept = jnp.dot(normed, w_recept, preferred_element_type=jnp.float32).astype(jnp.bfloat16)
    keys = jnp.dot(normed, w_keys, preferred_element_type=jnp.float32).astype(jnp.bfloat16)
    vals = jnp.dot(normed, w_values, preferred_element_type=jnp.float32).astype(jnp.bfloat16)
    decay_low = jnp.tanh(jnp.dot(normed, decay_first_matrix, preferred_element_type=jnp.float32)).astype(jnp.bfloat16)
    rate_low = jnp.dot(normed, rate_first_matrix, preferred_element_type=jnp.float32).astype(jnp.bfloat16)
    pre = decay_base + jnp.dot(decay_low, decay_second_matrix, preferred_element_type=jnp.float32)
    decay = jnp.exp(-jnp.exp(-jax.nn.softplus(-pre) - 0.5))
    rate = jax.nn.sigmoid(rate_base + jnp.dot(rate_low, rate_second_matrix, preferred_element_type=jnp.float32))

    def split_heads(values):
        return values.astype(jnp.float32).reshape(count, heads, width)
    r_head = split_heads(recept)
    k_head = split_heads(keys)
    v_head = split_heads(vals)
    d_head = split_heads(decay)
    a_head = split_heads(rate)
    unit = k_head * lax.rsqrt(lax.optimization_barrier(jnp.sum(k_head * k_head, axis=-1, keepdims=True)) + 1e-06)
    probe = jnp.einsum('bhvk,bhk->bhv', state, unit, precision=lax.Precision.HIGHEST)
    updated = state * d_head[:, :, None, :] - probe[..., None] * (unit * a_head)[:, :, None, :] + v_head[..., None] * k_head[:, :, None, :]
    mixed = jnp.einsum('bhvk,bhk->bhv', updated, r_head, precision=lax.Precision.HIGHEST)
    centre = mixed - lax.optimization_barrier(jnp.mean(mixed, axis=-1, keepdims=True))
    spread = lax.optimization_barrier(jnp.mean(centre * centre, axis=-1, keepdims=True))
    mixed = centre * lax.rsqrt(spread + 0.00064)
    mixed = (mixed.reshape(count, heads * width) * head_gain).astype(jnp.bfloat16)
    after = resid + jnp.dot(mixed, w_output, preferred_element_type=jnp.float32)
    return (after, updated)

def expert_part(rows, gate_w, up_w, down_w):
    gate = jnp.dot(rows, gate_w, preferred_element_type=jnp.float32)
    upper = jnp.dot(rows, up_w, preferred_element_type=jnp.float32)
    hidden = (jax.nn.silu(gate) * upper).astype(jnp.bfloat16)
    return jnp.dot(hidden, down_w, preferred_element_type=jnp.float32)

def reference(tokens, state, norm_gain, w_recept, w_keys, w_values, decay_base, decay_first_matrix, decay_second_matrix, rate_base, rate_first_matrix, rate_second_matrix, head_gain, w_output, second_gain, route_ids, route_weights, expert_gate, expert_up, expert_down):
    blocks_tok = tokens.reshape(N_EP, SEQ_DEV, MODEL_WIDTH)
    blocks_state = state.reshape((N_EP, SEQ_DEV) + state.shape[1:])

    def one_block(pair):
        return time_mixer(pair[0], pair[1], norm_gain, w_recept, w_keys, w_values, decay_base, decay_first_matrix, decay_second_matrix, rate_base, rate_first_matrix, rate_second_matrix, head_gain, w_output)
    after, new_state = lax.map(one_block, (blocks_tok, blocks_state))
    after = after.reshape(BATCH, MODEL_WIDTH)
    new_state = new_state.reshape(state.shape)
    second = norm_rows(after, second_gain).astype(jnp.bfloat16)
    gates_all = expert_gate.reshape(MODEL_WIDTH, EXPERTS, FF_E).transpose(1, 0, 2)
    ups_all = expert_up.reshape(MODEL_WIDTH, EXPERTS, FF_E).transpose(1, 0, 2)
    downs_all = expert_down.reshape(EXPERTS, FF_E, MODEL_WIDTH)
    limit = N_EP * CAP_DEV

    def one_expert(total, inputs):
        which, gate_w, up_w, down_w = inputs
        hit = route_ids == which
        member = jnp.any(hit, axis=1)
        share = lax.optimization_barrier(jnp.sum(jnp.where(hit, route_weights, 0.0), axis=1))
        picked = jnp.nonzero(member, size=limit, fill_value=0)[0].astype(jnp.int32)
        valid = (jnp.arange(limit, dtype=jnp.int32) < jnp.sum(member.astype(jnp.int32))).astype(jnp.float32)
        result = expert_part(second[picked], gate_w, up_w, down_w)
        total = total.at[picked].add((share[picked] * valid)[:, None] * result)
        return (total, None)
    blend, _ = lax.scan(one_expert, jnp.zeros((BATCH, MODEL_WIDTH), jnp.float32), (jnp.arange(EXPERTS, dtype=jnp.int32), gates_all, ups_all, downs_all))
    layer_out = (after + blend).astype(jnp.bfloat16)
    return (layer_out, new_state)
```

```python
import functools

import jax
import jax.numpy as jnp
from jax import lax
from jax.experimental import pallas as pl
from jax.experimental.pallas import tpu as pltpu
from jax.sharding import PartitionSpec as P

EXPERTS = 16
CAP_DEV = 6
ROWS = 8
SPLIT = 3

F32 = jnp.float32
BF16 = jnp.bfloat16
HBM = pl.BlockSpec(memory_space=pltpu.HBM)
VMEM = pl.BlockSpec(memory_space=pltpu.VMEM)
SMEM = pl.BlockSpec(memory_space=pltpu.SMEM)


def pin(value):
    return pltpu.with_memory_space_constraint(value, pltpu.HBM)


def iota(shape, dim):
    return lax.broadcasted_iota(jnp.int32, shape, dim)


def dot(a, b):
    return jnp.dot(a, b, preferred_element_type=F32)


def dot_t(a, b):
    return lax.dot_general(a, b, (((0,), (0,)), ((), ())), preferred_element_type=F32)


def head_sums(x):
    low = iota(x.shape, 1) < 64
    first = jnp.sum(jnp.where(low, x, 0.0), axis=1, keepdims=True)
    other = jnp.sum(jnp.where(low, 0.0, x), axis=1, keepdims=True)
    return jnp.where(low, first, other)


def mixer_kernel(
    start,
    tokens_in,
    norm_gain_in,
    decay_base_in,
    rate_base_in,
    head_gain_in,
    second_gain_in,
    ids_in,
    weights_in,
    state,
    w_recept,
    w_keys,
    w_values,
    decay_first,
    decay_second,
    rate_first,
    rate_second,
    w_output,
    packed,
    after_out,
    combine,
    terms_out,
    s_buf,
    wr_buf,
    wk_buf,
    wv_buf,
    d1_buf,
    d2_buf,
    r1_buf,
    r2_buf,
    wo_buf,
    lhs_buf,
    sums,
    tokens,
    norm_gain,
    decay_base,
    rate_base,
    head_gain,
    second_gain,
    ids_t,
    weights_t,
    w_sem,
    s_sem,
    a_sem,
):
    keys_out, vals_out, decay_out, ua_out, probe_out = (terms_out.at[i] for i in range(5))
    rows, width = tokens.shape
    small = [
        pltpu.make_async_copy(src, dst, a_sem.at[i])
        for i, (src, dst) in enumerate(
            (
                (tokens_in, tokens),
                (norm_gain_in, norm_gain),
                (ids_in, ids_t),
                (weights_in, weights_t),
                (decay_base_in, decay_base),
                (rate_base_in, rate_base),
                (head_gain_in, head_gain),
                (second_gain_in, second_gain),
            )
        )
    ]
    for copy in small:
        copy.start()
    heads = state.shape[1]
    chan = heads * 64
    groups = s_sem.shape[0]
    step = heads // groups
    pairs = heads // 2

    def weight(i, src, dst):
        return pltpu.make_async_copy(src, dst, w_sem.at[i])

    def state_copy(g):
        return pltpu.make_async_copy(
            state.at[:, pl.ds(g * step, step)], s_buf.at[:, pl.ds(g * step, step)], s_sem.at[g]
        )

    k_copy = weight(0, w_keys, wk_buf)
    d1_copy = weight(1, decay_first, d1_buf)
    r1_copy = weight(2, rate_first, r1_buf)
    d2_copy = weight(3, decay_second, d2_buf)
    r2_copy = weight(4, rate_second, r2_buf)
    r_copy = weight(5, w_recept, wr_buf)
    v_copy = weight(6, w_values, wv_buf)
    half = chan // 2
    o_copies = [
        weight(7 + i, w_output.at[pl.ds(i * half, half)], wo_buf.at[pl.ds(i * half, half)])
        for i in range(2)
    ]
    for copy in (k_copy, d1_copy, r1_copy, d2_copy, r2_copy, r_copy):
        copy.start()

    for copy in small:
        copy.wait()

    all_rows = ids_t.shape[1]
    pick = (iota((all_rows, rows), 0) == iota((all_rows, rows), 1) + start[0]).astype(F32)
    own_ids = jnp.dot(ids_t[...].astype(F32), pick, preferred_element_type=F32)
    own_weights = jnp.dot(
        weights_t[...], pick, preferred_element_type=F32, precision=lax.Precision.HIGHEST
    )
    expert = iota((EXPERTS, rows), 0).astype(F32)
    hit0 = own_ids[0:1] == expert
    hit1 = own_ids[1:2] == expert
    member = jnp.where(hit0 | hit1, 1.0, 0.0)
    share = jnp.where(hit0, own_weights[0:1], 0.0) + jnp.where(hit1, own_weights[1:2], 0.0)
    before = (iota((rows, rows), 0) < iota((rows, rows), 1)).astype(F32)
    order = dot(member, before)
    spread = (iota((EXPERTS * ROWS, EXPERTS), 0) // ROWS == iota((EXPERTS * ROWS, EXPERTS), 1))
    spread = spread.astype(F32)
    member_r = dot(spread, member) > 0.5
    order_r = dot(spread, order).astype(jnp.int32)
    share_r = jnp.dot(spread, share, preferred_element_type=F32, precision=lax.Precision.HIGHEST)
    row = iota((EXPERTS * ROWS, rows), 0) % ROWS
    tables = [jnp.where(member_r & (row < CAP_DEV) & (order_r == row), 1.0, 0.0)]
    for j in range(SPLIT):
        slot = SPLIT * (row - CAP_DEV) + j
        tables.append(jnp.where(member_r & (row >= CAP_DEV) & (order_r == slot), 1.0, 0.0))
    for j in range(SPLIT + 1):
        combine[j] = tables[j] * share_r

    resid = tokens[...].astype(F32)
    mean_sq = jnp.mean(resid * resid, axis=1, keepdims=True)
    normed = (resid * lax.rsqrt(mean_sq + 1e-06) * norm_gain[...]).astype(BF16)

    k_copy.wait()
    state_copy(0).start()
    keys_out[...] = dot(normed, wk_buf[...]).astype(BF16).astype(F32)
    d1_copy.wait()
    decay_low = jnp.tanh(dot(normed, d1_buf[...])).astype(BF16)
    r1_copy.wait()
    state_copy(1).start()
    rate_low = dot(normed, r1_buf[...]).astype(BF16)
    d2_copy.wait()
    pre = decay_base[...] + dot(decay_low, d2_buf[...])
    decay_out[...] = jnp.exp(-jnp.exp(-jax.nn.softplus(-pre) - 0.5))
    r2_copy.wait()
    rate = jax.nn.sigmoid(rate_base[...] + dot(rate_low, r2_buf[...]))
    r_copy.wait()
    for g in range(2, groups):
        state_copy(g).start()
    v_copy.start()
    recept = dot(normed, wr_buf[...]).astype(BF16).astype(F32)

    for p in range(pairs):
        at = slice(p * 128, p * 128 + 128)
        k = keys_out[:, at]
        unit = k * lax.rsqrt(head_sums(k * k) + 1e-06)
        ua = unit * rate[:, at]
        r = recept[:, at]
        dr = decay_out[:, at] * r
        ua_out[:, at] = ua
        sums[0, :, at] = head_sums(ua * r)
        sums[1, :, at] = head_sums(k * r)
        for h in range(2):
            lanes = slice(h * 64, h * 64 + 64)
            lhs_buf[2 * p + h, 0:rows] = unit[:, lanes]
            lhs_buf[2 * p + h, rows : 2 * rows] = dr[:, lanes]

    own_block = iota((rows, 128), 1) // 64 == iota((rows, 128), 0) % 2
    low = iota((rows, 128), 1) < 64
    token = iota((rows, 128), 0) // 2

    def diagonal(x):
        total = jnp.zeros((rows, 128), F32)
        for c in range(rows * 64 // 128):
            total = total + jnp.where(own_block & (token == c), x[:, c * 128 : c * 128 + 128], 0.0)
        return total + pltpu.roll(total, 64, 1)

    def state_step(g, carry):
        state_copy(g).wait()

        @pl.when(g == 1)
        def _():
            for copy in o_copies:
                copy.start()

        for p in range(step // 2):
            found = []
            for h in range(2):
                head = g * step + 2 * p + h
                block = s_buf[:, head].reshape(rows * 64, 64).astype(BF16)
                found.append(
                    lax.dot_general(
                        lhs_buf[head].astype(BF16),
                        block,
                        (((1,), (1,)), ((), ())),
                        preferred_element_type=F32,
                    )
                )
            at = pl.ds(pl.multiple_of((g * step + 2 * p) * 64, 128), 128)
            probe_out[:, at] = jnp.where(low, diagonal(found[0][:rows]), diagonal(found[1][:rows]))
            sums[2, :, at] = jnp.where(low, diagonal(found[0][rows:]), diagonal(found[1][rows:]))
        return carry

    lax.fori_loop(0, groups, state_step, 0)

    v_copy.wait()
    vals_out[...] = dot(normed, wv_buf[...]).astype(BF16).astype(F32)
    pieces = []
    for p in range(pairs):
        at = slice(p * 128, p * 128 + 128)
        mixed = sums[2, :, at] - probe_out[:, at] * sums[0, :, at] + vals_out[:, at] * sums[1, :, at]
        centre = mixed - head_sums(mixed) * (1.0 / 64)
        var = head_sums(centre * centre) * (1.0 / 64)
        pieces.append((centre * lax.rsqrt(var + 0.00064) * head_gain[:, at]).astype(BF16))
    mixed = jnp.concatenate(pieces, axis=1)
    after = resid
    for i in range(2):
        o_copies[i].wait()
        after = after + dot(mixed[:, i * half : i * half + half], wo_buf[pl.ds(i * half, half)])
    after_out[...] = after
    mean_sq = jnp.mean(after * after, axis=1, keepdims=True)
    second = (after * lax.rsqrt(mean_sq + 1e-06) * second_gain[...]).astype(BF16)
    piece = width // (SPLIT + 1)
    last = second[:, SPLIT * piece :]
    for j in range(SPLIT):
        packed[:, j * piece : (j + 1) * piece] = (
            dot(tables[0].astype(BF16), second[:, j * piece : (j + 1) * piece])
            + dot(tables[1 + j].astype(BF16), last)
        ).astype(BF16)


def mixer(start, args, state, mats):
    rows, width = args[0].shape
    heads = state.shape[1]
    chan = heads * 64
    low = mats[3].shape[1]
    groups = 4
    f = lambda *s: jax.ShapeDtypeStruct(s, F32)
    v = pltpu.VMEM
    return pl.pallas_call(
        mixer_kernel,
        out_shape=(
            jax.ShapeDtypeStruct((EXPERTS * ROWS, width * SPLIT // (SPLIT + 1)), BF16),
            f(rows, width),
            f(SPLIT + 1, EXPERTS * ROWS, rows),
            f(5, rows, chan),
        ),
        in_specs=[SMEM] + [HBM] * (len(args) + 1 + len(mats)),
        out_specs=(VMEM,) * 4,
        scratch_shapes=[
            v(state.shape, F32),
            v((width, chan), BF16),
            v((width, chan), BF16),
            v((width, chan), BF16),
            v((width, low), BF16),
            v((low, chan), BF16),
            v((width, low), BF16),
            v((low, chan), BF16),
            v((chan, width), BF16),
            v((heads, 2 * rows, 64), F32),
            v((3, rows, chan), F32),
            *(v(a.shape, a.dtype) for a in args),
            pltpu.SemaphoreType.DMA((9,)),
            pltpu.SemaphoreType.DMA((groups,)),
            pltpu.SemaphoreType.DMA((len(args),)),
        ],
        compiler_params=pltpu.CompilerParams(vmem_limit_bytes=67_000_000),
        cost_estimate=pl.CostEstimate(
            flops=24_000_000_000, bytes_accessed=30_000_000, transcendentals=200_000
        ),
        name="mixer",
    )(start, *map(pin, (*args, state, *mats)))


def update_kernel(
    state,
    terms_in,
    out,
    buf,
    lhs,
    in_sem,
    out_sem,
    terms,
    t_sem,
):
    keys, vals, decay, ua, probe = (terms.at[i] for i in range(5))
    terms_copy = pltpu.make_async_copy(terms_in, terms, t_sem.at[0])
    terms_copy.start()
    rows, heads = buf.shape[0], buf.shape[1]
    pairs = heads // 2

    def load(p):
        at = pl.ds(p * 2, 2)
        return pltpu.make_async_copy(state.at[:, at], buf.at[:, at], in_sem.at[p])

    def store(p):
        at = pl.ds(p * 2, 2)
        return pltpu.make_async_copy(buf.at[:, at], out.at[:, at], out_sem.at[p])

    for p in range(pairs):
        load(p).start()

    column = iota((64, 4 * rows), 1) % rows
    terms_copy.wait()

    def body(p, carry):
        lanes = pl.ds(pl.multiple_of(p * 128, 128), 128)
        d = decay[:, lanes]
        u, q = ua[:, lanes], probe[:, lanes]
        u_high = u.astype(BF16).astype(F32)
        q_high = q.astype(BF16).astype(F32)
        left = jnp.concatenate([vals[:, lanes], q_high, q - q_high, q_high], axis=0).T
        right = jnp.concatenate([keys[:, lanes], -u_high, -u_high, u_high - u], axis=0)
        load(p).wait()
        for h in range(2):
            part = left[h * 64 : h * 64 + 64]
            for b in range(rows):
                lhs[h, b * 64 : b * 64 + 64] = jnp.where(column == b, part, 0.0).astype(BF16)
            if h:
                right = pltpu.roll(right, 64, 1)
                d = pltpu.roll(d, 64, 1)
            change = dot(lhs[h], right[:, :64].astype(BF16))
            for b in range(rows):
                buf[b, 2 * p + h] = (
                    buf[b, 2 * p + h] * d[b : b + 1, :64] + change[b * 64 : b * 64 + 64]
                )
        store(p).start()
        return carry

    lax.fori_loop(0, pairs, body, 0)
    for p in range(pairs):
        store(p).wait()


def update(state, terms):
    pairs = state.shape[1] // 2
    return pl.pallas_call(
        update_kernel,
        out_shape=jax.ShapeDtypeStruct(state.shape, F32),
        in_specs=[HBM] * 2,
        out_specs=HBM,
        scratch_shapes=[
            pltpu.VMEM(state.shape, F32),
            pltpu.VMEM((2, state.shape[0] * 64, 4 * state.shape[0]), BF16),
            pltpu.SemaphoreType.DMA((pairs,)),
            pltpu.SemaphoreType.DMA((pairs,)),
            pltpu.VMEM(terms.shape, F32),
            pltpu.SemaphoreType.DMA((1,)),
        ],
        compiler_params=pltpu.CompilerParams(vmem_limit_bytes=67_000_000),
        cost_estimate=pl.CostEstimate(
            flops=16_000_000_000, bytes_accessed=26_000_000, transcendentals=0
        ),
        name="update",
    )(pin(state), pin(terms))


def expert_kernel(chunk, group, *refs):
    received = refs[:group]
    gate, up, down = refs[group : group + 3]
    results = refs[group + 3 : 2 * group + 3]
    x_buf, acc = refs[2 * group + 3 :]
    width, hidden = gate.shape
    steps = hidden // chunk
    piece = width // (SPLIT + 1)
    slots = EXPERTS * CAP_DEV
    packed_rows = EXPERTS * ROWS

    source, c = iota((slots, packed_rows), 0) // CAP_DEV, iota((slots, packed_rows), 0) % CAP_DEV
    column = iota((slots, packed_rows), 1)
    tables = [jnp.where(column == source * ROWS + c, 1.0, 0.0).astype(BF16)]
    for j in range(SPLIT):
        here = (column == source * ROWS + CAP_DEV + c // SPLIT) & (c % SPLIT == j)
        tables.append(jnp.where(here, 1.0, 0.0).astype(BF16))
    for m in range(group):
        at = slice(m * slots, (m + 1) * slots)
        value = received[m][...]
        x_buf[at, : SPLIT * piece] = dot(tables[0], value).astype(BF16)
        x_buf[at, SPLIT * piece :] = sum(
            dot(tables[1 + j], value[:, j * piece : (j + 1) * piece]) for j in range(SPLIT)
        ).astype(BF16)

    for i in range(steps):
        at = slice(i * chunk, (i + 1) * chunk)
        x = x_buf[...]
        g = dot(x, gate[:, at])
        u = dot(x, up[:, at])
        h = (jax.nn.silu(g) * u).astype(BF16)
        y = dot(h, down[at])
        acc[...] = y if i == 0 else acc[...] + y

    for m in range(group):
        y = acc[m * slots : (m + 1) * slots].astype(BF16)
        last = y[:, SPLIT * piece :]
        for j in range(SPLIT):
            results[m][:, j * piece : (j + 1) * piece] = (
                dot_t(tables[0], y[:, j * piece : (j + 1) * piece]) + dot_t(tables[1 + j], last)
            ).astype(BF16)


def experts(received, gate, up, down):
    group = len(received)
    width, hidden = gate.shape
    chunk = 256 if hidden % 256 == 0 else 128
    rows = group * EXPERTS * CAP_DEV
    return pl.pallas_call(
        functools.partial(expert_kernel, chunk, group),
        out_shape=tuple(jax.ShapeDtypeStruct(r.shape, BF16) for r in received),
        in_specs=[VMEM] * (group + 3),
        out_specs=(VMEM,) * group,
        scratch_shapes=[
            pltpu.VMEM((rows, width), BF16),
            pltpu.VMEM((rows, width), F32),
        ],
        compiler_params=pltpu.CompilerParams(vmem_limit_bytes=12 * 1024 * 1024),
        cost_estimate=pl.CostEstimate(
            flops=6 * rows * width * hidden, bytes_accessed=6 * width * hidden, transcendentals=0
        ),
        name="experts",
    )(*received, gate, up, down)


def window(value):
    return pl.pallas_call(
        lambda source, out: None,
        out_shape=jax.ShapeDtypeStruct(value.shape, value.dtype),
        in_specs=[HBM],
        out_specs=HBM,
        input_output_aliases={0: 0},
        compiler_params=pltpu.CompilerParams(vmem_limit_bytes=1024 * 1024),
        cost_estimate=pl.CostEstimate(
            flops=40_000_000_000, bytes_accessed=1024, transcendentals=0
        ),
        name="window",
    )(pin(value))


def combine_kernel(returned, after, combine, out):
    width = after.shape[1]
    piece = width // (SPLIT + 1)

    def blend(table, value):
        high = table.astype(BF16)
        low = (table - high.astype(F32)).astype(BF16)
        return dot_t(high, value) + dot_t(low, value)

    value = returned[...]
    first = blend(combine[0], value)
    last = sum(
        blend(combine[1 + j], value[:, j * piece : (j + 1) * piece]) for j in range(SPLIT)
    )
    at = SPLIT * piece
    out[:, :at] = (after[:, :at] + first).astype(BF16)
    out[:, at:] = (after[:, at:] + last).astype(BF16)


def on_device(
    tokens,
    state,
    norm_gain,
    w_recept,
    w_keys,
    w_values,
    decay_base,
    decay_first_matrix,
    decay_second_matrix,
    rate_base,
    rate_first_matrix,
    rate_second_matrix,
    head_gain,
    w_output,
    second_gain,
    route_ids,
    route_weights,
    expert_gate,
    expert_up,
    expert_down,
):
    devices = lax.axis_size("ep")
    group = devices // EXPERTS
    rows = tokens.shape[0]
    start = (lax.axis_index("ep") * rows).astype(jnp.int32).reshape(1)
    line = lambda a: a.reshape(1, -1)
    packed, after, combine, terms = mixer(
        start,
        (
            tokens,
            line(norm_gain),
            line(decay_base),
            line(rate_base),
            line(head_gain),
            line(second_gain),
            route_ids.T,
            route_weights.T,
        ),
        state,
        (
            w_recept,
            w_keys,
            w_values,
            decay_first_matrix,
            decay_second_matrix,
            rate_first_matrix,
            rate_second_matrix,
            w_output,
        ),
    )
    peers = [[e * group + j for e in range(EXPERTS)] for j in range(group)]
    cols = packed.shape[1]

    def exchange(value):
        chunks = value.reshape(EXPERTS, ROWS, cols)
        out = lax.all_to_all(
            chunks, "ep", split_axis=0, concat_axis=0, tiled=True, axis_index_groups=peers
        )
        return out.reshape(EXPERTS * ROWS, cols)

    def turn(value, by):
        return lax.ppermute(
            value,
            "ep",
            [(i, i // group * group + (i % group + by) % group) for i in range(devices)],
        )

    own = exchange(window(packed))
    new_state = update(state, terms)
    received = (own,) + tuple(turn(own, by) for by in range(1, group))
    results = experts(received, expert_gate, expert_up, expert_down)
    total = results[0].astype(F32)
    for by in range(1, group):
        total = total + turn(results[by], group - by).astype(F32)
    returned = exchange(total.astype(BF16))
    layer_out = pl.pallas_call(
        combine_kernel,
        out_shape=jax.ShapeDtypeStruct(after.shape, BF16),
        in_specs=[VMEM] * 3,
        out_specs=VMEM,
        name="combine",
    )(returned, after, combine)
    return (layer_out, new_state)


def solution(mesh):
    in_specs = (
        P("ep", None),
        P("ep", None, None, None),
        P(),
        P(),
        P(),
        P(),
        P(),
        P(),
        P(),
        P(),
        P(),
        P(),
        P(),
        P(),
        P(),
        P(),
        P(),
        P(None, "ep"),
        P(None, "ep"),
        P("ep", None),
    )
    out_specs = (P("ep", None), P("ep", None, None, None))
    return jax.shard_map(
        on_device, mesh=mesh, in_specs=in_specs, out_specs=out_specs, check_vma=False
    )
```

```python
import functools

import jax
import jax.numpy as jnp
from jax import lax
from jax.experimental import pallas as pl
from jax.experimental.pallas import tpu as pltpu
from jax.sharding import PartitionSpec as P

EXPERTS = 16
CAP_DEV = 6
ROWS = 8
SPLIT = 3

F32 = jnp.float32
BF16 = jnp.bfloat16
HBM = pl.BlockSpec(memory_space=pltpu.HBM)
VMEM = pl.BlockSpec(memory_space=pltpu.VMEM)
SMEM = pl.BlockSpec(memory_space=pltpu.SMEM)


def pin(value):
    return pltpu.with_memory_space_constraint(value, pltpu.HBM)


def iota(shape, dim):
    return lax.broadcasted_iota(jnp.int32, shape, dim)


def dot(a, b):
    return jnp.dot(a, b, preferred_element_type=F32)


def dot_t(a, b):
    return lax.dot_general(a, b, (((0,), (0,)), ((), ())), preferred_element_type=F32)


def head_sums(x):
    low = iota(x.shape, 1) < 64
    first = jnp.sum(jnp.where(low, x, 0.0), axis=1, keepdims=True)
    other = jnp.sum(jnp.where(low, 0.0, x), axis=1, keepdims=True)
    return jnp.where(low, first, other)


def mixer_kernel(
    start,
    tokens_in,
    norm_gain_in,
    decay_base_in,
    rate_base_in,
    head_gain_in,
    second_gain_in,
    ids_in,
    weights_in,
    state,
    w_recept,
    w_keys,
    w_values,
    decay_first,
    decay_second,
    rate_first,
    rate_second,
    w_output,
    packed_out,
    after,
    combine,
    terms_out,
    packed,
    terms,
    s_buf,
    wr_buf,
    wk_buf,
    wv_buf,
    d1_buf,
    d2_buf,
    r1_buf,
    r2_buf,
    wo_buf,
    lhs_buf,
    sums,
    tokens,
    norm_gain,
    decay_base,
    rate_base,
    head_gain,
    second_gain,
    ids_t,
    weights_t,
    w_sem,
    s_sem,
    a_sem,
    o_sem,
):
    keys_out, vals_out, decay_out, ua_out, probe_out = (terms.at[i] for i in range(5))
    rows, width = tokens.shape
    small = [
        pltpu.make_async_copy(src, dst, a_sem.at[i])
        for i, (src, dst) in enumerate(
            (
                (tokens_in, tokens),
                (norm_gain_in, norm_gain),
                (ids_in, ids_t),
                (weights_in, weights_t),
                (decay_base_in, decay_base),
                (rate_base_in, rate_base),
                (head_gain_in, head_gain),
                (second_gain_in, second_gain),
            )
        )
    ]
    for copy in small:
        copy.start()
    heads = state.shape[1]
    chan = heads * 64
    groups = s_sem.shape[0]
    step = heads // groups
    pairs = heads // 2

    def weight(i, src, dst):
        return pltpu.make_async_copy(src, dst, w_sem.at[i])

    def state_copy(g):
        return pltpu.make_async_copy(
            state.at[:, pl.ds(g * step, step)], s_buf.at[:, pl.ds(g * step, step)], s_sem.at[g]
        )

    k_copy = weight(0, w_keys, wk_buf)
    d1_copy = weight(1, decay_first, d1_buf)
    r1_copy = weight(2, rate_first, r1_buf)
    d2_copy = weight(3, decay_second, d2_buf)
    r2_copy = weight(4, rate_second, r2_buf)
    r_copy = weight(5, w_recept, wr_buf)
    v_copy = weight(6, w_values, wv_buf)
    half = chan // 2
    o_copies = [
        weight(7 + i, w_output.at[pl.ds(i * half, half)], wo_buf.at[pl.ds(i * half, half)])
        for i in range(2)
    ]
    k_copy.start()
    for copy in small:
        copy.wait()

    resid = tokens[...].astype(F32)
    mean_sq = jnp.mean(resid * resid, axis=1, keepdims=True)
    normed = (resid * lax.rsqrt(mean_sq + 1e-06) * norm_gain[...]).astype(BF16)

    for copy in (d1_copy, r1_copy, d2_copy, r2_copy, r_copy):
        copy.start()
    k_copy.wait()
    v_copy.start()
    keys_out[...] = dot(normed, wk_buf[...]).astype(BF16).astype(F32)
    for copy in (d1_copy, r1_copy, d2_copy, r2_copy):
        copy.wait()
    decay_low = jnp.tanh(dot(normed, d1_buf[...])).astype(BF16)
    rate_low = dot(normed, r1_buf[...]).astype(BF16)
    pre = decay_base[...] + dot(decay_low, d2_buf[...])
    decay_out[...] = jnp.exp(-jnp.exp(-jax.nn.softplus(-pre) - 0.5))
    rate = jax.nn.sigmoid(rate_base[...] + dot(rate_low, r2_buf[...]))
    state_copy(0).start()
    r_copy.wait()
    state_copy(1).start()
    recept = dot(normed, wr_buf[...]).astype(BF16).astype(F32)
    v_copy.wait()
    for g in range(2, groups):
        state_copy(g).start()
    all_rows = ids_t.shape[1]
    pick = (iota((all_rows, rows), 0) == iota((all_rows, rows), 1) + start[0]).astype(F32)
    own_ids = jnp.dot(ids_t[...].astype(F32), pick, preferred_element_type=F32)
    own_weights = jnp.dot(
        weights_t[...], pick, preferred_element_type=F32, precision=lax.Precision.HIGHEST
    )
    expert = iota((EXPERTS, rows), 0).astype(F32)
    hit0 = own_ids[0:1] == expert
    hit1 = own_ids[1:2] == expert
    member = jnp.where(hit0 | hit1, 1.0, 0.0)
    share = jnp.where(hit0, own_weights[0:1], 0.0) + jnp.where(hit1, own_weights[1:2], 0.0)
    before = (iota((rows, rows), 0) < iota((rows, rows), 1)).astype(F32)
    order = dot(member, before)
    spread = (iota((EXPERTS * ROWS, EXPERTS), 0) // ROWS == iota((EXPERTS * ROWS, EXPERTS), 1))
    spread = spread.astype(F32)
    member_r = dot(spread, member) > 0.5
    order_r = dot(spread, order).astype(jnp.int32)
    share_r = jnp.dot(spread, share, preferred_element_type=F32, precision=lax.Precision.HIGHEST)
    row = iota((EXPERTS * ROWS, rows), 0) % ROWS
    tables = [jnp.where(member_r & (row < CAP_DEV) & (order_r == row), 1.0, 0.0)]
    for j in range(SPLIT):
        slot = SPLIT * (row - CAP_DEV) + j
        tables.append(jnp.where(member_r & (row >= CAP_DEV) & (order_r == slot), 1.0, 0.0))
    for j in range(SPLIT + 1):
        combine[j] = (tables[j] * share_r).T

    vals_out[...] = dot(normed, wv_buf[...]).astype(BF16).astype(F32)

    for p in range(pairs):
        at = slice(p * 128, p * 128 + 128)
        k = keys_out[:, at]
        unit = k * lax.rsqrt(head_sums(k * k) + 1e-06)
        ua = unit * rate[:, at]
        r = recept[:, at]
        dr = decay_out[:, at] * r
        ua_out[:, at] = ua
        sums[0, :, at] = head_sums(ua * r)
        sums[1, :, at] = head_sums(k * r)
        for h in range(2):
            lanes = slice(h * 64, h * 64 + 64)
            lhs_buf[2 * p + h, 0:rows] = unit[:, lanes]
            lhs_buf[2 * p + h, rows : 2 * rows] = dr[:, lanes]

    own_block = iota((rows, 128), 1) // 64 == iota((rows, 128), 0) % 2
    low = iota((rows, 128), 1) < 64
    token = iota((rows, 128), 0) // 2

    def diagonal(x):
        total = jnp.zeros((rows, 128), F32)
        for c in range(rows * 64 // 128):
            total = total + jnp.where(own_block & (token == c), x[:, c * 128 : c * 128 + 128], 0.0)
        return total + pltpu.roll(total, 64, 1)

    def read_out(g):
        for p in range(g * step // 2, (g + 1) * step // 2):
            at = slice(p * 128, p * 128 + 128)
            found = []
            for head in (2 * p, 2 * p + 1):
                block = s_buf[:, head].reshape(rows * 64, 64).astype(BF16)
                found.append(
                    lax.dot_general(
                        lhs_buf[head].astype(BF16),
                        block,
                        (((1,), (1,)), ((), ())),
                        preferred_element_type=F32,
                    )
                )
            probe_out[:, at] = jnp.where(low, diagonal(found[0][:rows]), diagonal(found[1][:rows]))
            sums[2, :, at] = jnp.where(low, diagonal(found[0][rows:]), diagonal(found[1][rows:]))

    def normalized(p):
        at = slice(p * 128, p * 128 + 128)
        mixed = sums[2, :, at] - probe_out[:, at] * sums[0, :, at]
        mixed = mixed + vals_out[:, at] * sums[1, :, at]
        centre = mixed - head_sums(mixed) * (1.0 / 64)
        var = head_sums(centre * centre) * (1.0 / 64)
        return (centre * lax.rsqrt(var + 0.00064) * head_gain[:, at]).astype(BF16)

    pieces = []
    for g in range(groups):
        state_copy(g).wait()
        if g == 0:
            for copy in o_copies:
                copy.start()
        read_out(g)
        if g:
            pieces += [normalized(p) for p in range((g - 1) * step // 2, g * step // 2)]
    pieces += [normalized(p) for p in range((groups - 1) * step // 2, pairs)]
    mixed = jnp.concatenate(pieces, axis=1)
    total = resid
    for i in range(2):
        o_copies[i].wait()
        total = total + dot(mixed[:, i * half : i * half + half], wo_buf[pl.ds(i * half, half)])
    after[...] = total
    terms_copy = pltpu.make_async_copy(terms, terms_out, o_sem.at[0])
    terms_copy.start()

    mean_sq = jnp.mean(total * total, axis=1, keepdims=True)
    second = (total * lax.rsqrt(mean_sq + 1e-06) * second_gain[...]).astype(BF16)
    piece = width // (SPLIT + 1)
    last = second[:, SPLIT * piece :]
    copies = []
    for j in range(SPLIT):
        at = slice(j * piece, (j + 1) * piece)
        packed[:, at] = (
            dot(tables[0].astype(BF16), second[:, at]) + dot(tables[1 + j].astype(BF16), last)
        ).astype(BF16)
        at = pl.ds(j * piece, piece)
        copies.append(
            pltpu.make_async_copy(packed.at[:, at], packed_out.at[:, at], o_sem.at[1 + j])
        )
        copies[j].start()
    terms_copy.wait()
    for copy in copies:
        copy.wait()


def mixer(start, args, state, mats):
    rows, width = args[0].shape
    heads = state.shape[1]
    chan = heads * 64
    low = mats[3].shape[1]
    groups = 4
    f = lambda *s: jax.ShapeDtypeStruct(s, F32)
    v = pltpu.VMEM
    return pl.pallas_call(
        mixer_kernel,
        out_shape=(
            pltpu.HBM((EXPERTS * ROWS, width * SPLIT // (SPLIT + 1)), BF16),
            f(rows, width),
            f(SPLIT + 1, rows, EXPERTS * ROWS),
            pltpu.HBM((5, rows, chan), F32),
        ),
        in_specs=[SMEM] + [HBM] * (len(args) + 1 + len(mats)),
        out_specs=(HBM, VMEM, VMEM, HBM),
        scratch_shapes=[
            v((EXPERTS * ROWS, width * SPLIT // (SPLIT + 1)), BF16),
            v((5, rows, chan), F32),
            v(state.shape, F32),
            v((width, chan), BF16),
            v((width, chan), BF16),
            v((width, chan), BF16),
            v((width, low), BF16),
            v((low, chan), BF16),
            v((width, low), BF16),
            v((low, chan), BF16),
            v((chan, width), BF16),
            v((heads, 2 * rows, 64), F32),
            v((3, rows, chan), F32),
            *(v(a.shape, a.dtype) for a in args),
            pltpu.SemaphoreType.DMA((9,)),
            pltpu.SemaphoreType.DMA((groups,)),
            pltpu.SemaphoreType.DMA((len(args),)),
            pltpu.SemaphoreType.DMA((1 + SPLIT,)),
        ],
        compiler_params=pltpu.CompilerParams(vmem_limit_bytes=67_000_000),
        cost_estimate=pl.CostEstimate(
            flops=24_000_000_000, bytes_accessed=30_000_000, transcendentals=200_000
        ),
        name="mixer",
    )(start, *map(pin, (*args, state, *mats)))


def update_kernel(
    state,
    terms_in,
    out,
    buf,
    lhs,
    in_sem,
    out_sem,
    terms,
    t_sem,
):
    keys, vals, decay, ua, probe = (terms.at[i] for i in range(5))
    terms_copy = pltpu.make_async_copy(terms_in, terms, t_sem.at[0])
    terms_copy.start()
    rows, heads = buf.shape[0], buf.shape[1]
    pairs = heads // 2

    def load(p):
        at = pl.ds(p * 2, 2)
        return pltpu.make_async_copy(state.at[:, at], buf.at[:, at], in_sem.at[p])

    def store(p):
        at = pl.ds(p * 2, 2)
        return pltpu.make_async_copy(buf.at[:, at], out.at[:, at], out_sem.at[p])

    for p in range(pairs):
        load(p).start()

    column = iota((64, 4 * rows), 1) % rows
    terms_copy.wait()

    def body(p, carry):
        lanes = pl.ds(pl.multiple_of(p * 128, 128), 128)
        d = decay[:, lanes]
        u, q = ua[:, lanes], probe[:, lanes]
        u_high = u.astype(BF16).astype(F32)
        q_high = q.astype(BF16).astype(F32)
        left = jnp.concatenate([vals[:, lanes], q_high, q - q_high, q_high], axis=0).T
        right = jnp.concatenate([keys[:, lanes], -u_high, -u_high, u_high - u], axis=0)
        load(p).wait()
        for h in range(2):
            part = left[h * 64 : h * 64 + 64]
            for b in range(rows):
                lhs[h, b * 64 : b * 64 + 64] = jnp.where(column == b, part, 0.0).astype(BF16)
            if h:
                right = pltpu.roll(right, 64, 1)
                d = pltpu.roll(d, 64, 1)
            change = dot(lhs[h], right[:, :64].astype(BF16))
            for b in range(rows):
                buf[b, 2 * p + h] = (
                    buf[b, 2 * p + h] * d[b : b + 1, :64] + change[b * 64 : b * 64 + 64]
                )
        store(p).start()
        return carry

    lax.fori_loop(0, pairs, body, 0)
    for p in range(pairs):
        store(p).wait()


def update(state, terms):
    pairs = state.shape[1] // 2
    return pl.pallas_call(
        update_kernel,
        out_shape=jax.ShapeDtypeStruct(state.shape, F32),
        in_specs=[HBM] * 2,
        out_specs=HBM,
        scratch_shapes=[
            pltpu.VMEM(state.shape, F32),
            pltpu.VMEM((2, state.shape[0] * 64, 4 * state.shape[0]), BF16),
            pltpu.SemaphoreType.DMA((pairs,)),
            pltpu.SemaphoreType.DMA((pairs,)),
            pltpu.VMEM(terms.shape, F32),
            pltpu.SemaphoreType.DMA((1,)),
        ],
        compiler_params=pltpu.CompilerParams(vmem_limit_bytes=32 * 1024 * 1024),
        cost_estimate=pl.CostEstimate(
            flops=16_000_000_000, bytes_accessed=26_000_000, transcendentals=0
        ),
        name="update",
    )(pin(state), pin(terms))


def expert_kernel(chunk, group, *refs):
    received = refs[:group]
    gate, up, down = refs[group : group + 3]
    results = refs[group + 3 : 2 * group + 3]
    x_buf, acc = refs[2 * group + 3 :]
    width, hidden = gate.shape
    steps = hidden // chunk
    piece = width // (SPLIT + 1)
    slots = EXPERTS * CAP_DEV
    packed_rows = EXPERTS * ROWS

    source, c = iota((slots, packed_rows), 0) // CAP_DEV, iota((slots, packed_rows), 0) % CAP_DEV
    column = iota((slots, packed_rows), 1)
    tables = [jnp.where(column == source * ROWS + c, 1.0, 0.0).astype(BF16)]
    for j in range(SPLIT):
        here = (column == source * ROWS + CAP_DEV + c // SPLIT) & (c % SPLIT == j)
        tables.append(jnp.where(here, 1.0, 0.0).astype(BF16))
    for m in range(group):
        at = slice(m * slots, (m + 1) * slots)
        value = received[m][...]
        x_buf[at, : SPLIT * piece] = dot(tables[0], value).astype(BF16)
        x_buf[at, SPLIT * piece :] = sum(
            dot(tables[1 + j], value[:, j * piece : (j + 1) * piece]) for j in range(SPLIT)
        ).astype(BF16)

    for i in range(steps):
        at = slice(i * chunk, (i + 1) * chunk)
        x = x_buf[...]
        g = dot(x, gate[:, at])
        u = dot(x, up[:, at])
        h = (jax.nn.silu(g) * u).astype(BF16)
        y = dot(h, down[at])
        acc[...] = y if i == 0 else acc[...] + y

    for m in range(group):
        y = acc[m * slots : (m + 1) * slots].astype(BF16)
        last = y[:, SPLIT * piece :]
        for j in range(SPLIT):
            results[m][:, j * piece : (j + 1) * piece] = (
                dot_t(tables[0], y[:, j * piece : (j + 1) * piece]) + dot_t(tables[1 + j], last)
            ).astype(BF16)


def experts(received, gate, up, down):
    group = len(received)
    width, hidden = gate.shape
    chunk = 256 if hidden % 256 == 0 else 128
    rows = group * EXPERTS * CAP_DEV
    return pl.pallas_call(
        functools.partial(expert_kernel, chunk, group),
        out_shape=tuple(jax.ShapeDtypeStruct(r.shape, BF16) for r in received),
        in_specs=[VMEM] * (group + 3),
        out_specs=(VMEM,) * group,
        scratch_shapes=[
            pltpu.VMEM((rows, width), BF16),
            pltpu.VMEM((rows, width), F32),
        ],
        compiler_params=pltpu.CompilerParams(vmem_limit_bytes=12 * 1024 * 1024),
        cost_estimate=pl.CostEstimate(
            flops=6 * rows * width * hidden, bytes_accessed=6 * width * hidden, transcendentals=0
        ),
        name="experts",
    )(*received, gate, up, down)


def window(value):
    return pl.pallas_call(
        lambda source, out: None,
        out_shape=jax.ShapeDtypeStruct(value.shape, value.dtype),
        in_specs=[HBM],
        out_specs=HBM,
        input_output_aliases={0: 0},
        compiler_params=pltpu.CompilerParams(vmem_limit_bytes=1024 * 1024),
        cost_estimate=pl.CostEstimate(
            flops=40_000_000_000, bytes_accessed=1024, transcendentals=0
        ),
        name="window",
    )(pin(value))


def combine_kernel(returned, after, combine, out):
    width = after.shape[1]
    piece = width // (SPLIT + 1)

    def blend(table, value):
        high = table.astype(BF16)
        low = (table - high.astype(F32)).astype(BF16)
        return dot(high, value) + dot(low, value)

    value = returned[...]
    first = blend(combine[0], value)
    last = sum(
        blend(combine[1 + j], value[:, j * piece : (j + 1) * piece]) for j in range(SPLIT)
    )
    at = SPLIT * piece
    out[:, :at] = (after[:, :at] + first).astype(BF16)
    out[:, at:] = (after[:, at:] + last).astype(BF16)


def on_device(
    tokens,
    state,
    norm_gain,
    w_recept,
    w_keys,
    w_values,
    decay_base,
    decay_first_matrix,
    decay_second_matrix,
    rate_base,
    rate_first_matrix,
    rate_second_matrix,
    head_gain,
    w_output,
    second_gain,
    route_ids,
    route_weights,
    expert_gate,
    expert_up,
    expert_down,
):
    devices = lax.axis_size("ep")
    group = devices // EXPERTS
    rows = tokens.shape[0]
    start = (lax.axis_index("ep") * rows).astype(jnp.int32).reshape(1)
    line = lambda a: a.reshape(1, -1)
    packed, after, combine, terms = mixer(
        start,
        (
            tokens,
            line(norm_gain),
            line(decay_base),
            line(rate_base),
            line(head_gain),
            line(second_gain),
            route_ids.T,
            route_weights.T,
        ),
        state,
        (
            w_recept,
            w_keys,
            w_values,
            decay_first_matrix,
            decay_second_matrix,
            rate_first_matrix,
            rate_second_matrix,
            w_output,
        ),
    )
    peers = [[e * group + j for e in range(EXPERTS)] for j in range(group)]
    cols = packed.shape[1]

    def exchange(value):
        chunks = value.reshape(EXPERTS, ROWS, cols)
        out = lax.all_to_all(
            chunks, "ep", split_axis=0, concat_axis=0, tiled=True, axis_index_groups=peers
        )
        return out.reshape(EXPERTS * ROWS, cols)

    def turn(value, by):
        return lax.ppermute(
            value,
            "ep",
            [(i, i // group * group + (i % group + by) % group) for i in range(devices)],
        )

    own = exchange(window(packed))
    new_state = update(state, terms)
    received = (own,) + tuple(turn(own, by) for by in range(1, group))
    results = experts(received, expert_gate, expert_up, expert_down)
    total = results[0].astype(F32)
    for by in range(1, group):
        total = total + turn(results[by], group - by).astype(F32)
    returned = exchange(total.astype(BF16))
    layer_out = pl.pallas_call(
        combine_kernel,
        out_shape=jax.ShapeDtypeStruct(after.shape, BF16),
        in_specs=[VMEM] * 3,
        out_specs=VMEM,
        compiler_params=pltpu.CompilerParams(vmem_limit_bytes=8 * 1024 * 1024),
        name="combine",
    )(returned, after, combine)
    return (layer_out, new_state)


def solution(mesh):
    in_specs = (
        P("ep", None),
        P("ep", None, None, None),
        P(),
        P(),
        P(),
        P(),
        P(),
        P(),
        P(),
        P(),
        P(),
        P(),
        P(),
        P(),
        P(),
        P(),
        P(),
        P(None, "ep"),
        P(None, "ep"),
        P("ep", None),
    )
    out_specs = (P("ep", None), P("ep", None, None, None))
    return jax.shard_map(
        on_device, mesh=mesh, in_specs=in_specs, out_specs=out_specs, check_vma=False
    )
```

```python
import functools

import jax
import jax.numpy as jnp
from jax import lax
from jax.experimental import pallas as pl
from jax.experimental.pallas import tpu as pltpu
from jax.sharding import PartitionSpec as P

EXPERTS = 16
CAP_DEV = 6
ROWS = 8
SPLIT = 3

F32 = jnp.float32
BF16 = jnp.bfloat16
HBM = pl.BlockSpec(memory_space=pltpu.HBM)
VMEM = pl.BlockSpec(memory_space=pltpu.VMEM)
SMEM = pl.BlockSpec(memory_space=pltpu.SMEM)


def pin(value):
    return pltpu.with_memory_space_constraint(value, pltpu.HBM)


def iota(shape, dim):
    return lax.broadcasted_iota(jnp.int32, shape, dim)


def dot(a, b):
    return jnp.dot(a, b, preferred_element_type=F32)


def dot_t(a, b):
    return lax.dot_general(a, b, (((0,), (0,)), ((), ())), preferred_element_type=F32)


def head_sums(x):
    low = iota(x.shape, 1) < 64
    first = jnp.sum(jnp.where(low, x, 0.0), axis=1, keepdims=True)
    other = jnp.sum(jnp.where(low, 0.0, x), axis=1, keepdims=True)
    return jnp.where(low, first, other)


def mixer_kernel(
    start,
    tokens_in,
    norm_gain_in,
    decay_base_in,
    rate_base_in,
    head_gain_in,
    second_gain_in,
    ids_in,
    weights_in,
    state,
    w_recept,
    w_keys,
    w_values,
    decay_first,
    decay_second,
    rate_first,
    rate_second,
    w_output,
    packed_out,
    after,
    combine,
    terms_out,
    packed,
    terms,
    s_buf,
    wr_buf,
    wk_buf,
    wv_buf,
    d1_buf,
    d2_buf,
    r1_buf,
    r2_buf,
    wo_buf,
    lhs_buf,
    sums,
    tokens,
    norm_gain,
    decay_base,
    rate_base,
    head_gain,
    second_gain,
    ids_t,
    weights_t,
    w_sem,
    s_sem,
    a_sem,
    o_sem,
):
    keys_out, vals_out, decay_out, ua_out, probe_out = (terms.at[i] for i in range(5))
    rows, width = tokens.shape
    small = [
        pltpu.make_async_copy(src, dst, a_sem.at[i])
        for i, (src, dst) in enumerate(
            (
                (tokens_in, tokens),
                (norm_gain_in, norm_gain),
                (ids_in, ids_t),
                (weights_in, weights_t),
                (decay_base_in, decay_base),
                (rate_base_in, rate_base),
                (head_gain_in, head_gain),
                (second_gain_in, second_gain),
            )
        )
    ]
    for copy in small:
        copy.start()
    heads = state.shape[1]
    chan = heads * 64
    groups = s_sem.shape[0]
    step = heads // groups
    pairs = heads // 2

    def weight(i, src, dst):
        return pltpu.make_async_copy(src, dst, w_sem.at[i])

    def state_copy(g):
        return pltpu.make_async_copy(
            state.at[:, pl.ds(g * step, step)], s_buf.at[:, pl.ds(g * step, step)], s_sem.at[g]
        )

    k_copy = weight(0, w_keys, wk_buf)
    d1_copy = weight(1, decay_first, d1_buf)
    r1_copy = weight(2, rate_first, r1_buf)
    d2_copy = weight(3, decay_second, d2_buf)
    r2_copy = weight(4, rate_second, r2_buf)
    r_copy = weight(5, w_recept, wr_buf)
    v_copy = weight(6, w_values, wv_buf)
    half = chan // 2
    o_copies = [
        weight(7 + i, w_output.at[pl.ds(i * half, half)], wo_buf.at[pl.ds(i * half, half)])
        for i in range(2)
    ]
    for copy in (d1_copy, r1_copy, d2_copy, r2_copy, k_copy):
        copy.start()
    for copy in small:
        copy.wait()

    resid = tokens[...].astype(F32)
    mean_sq = jnp.mean(resid * resid, axis=1, keepdims=True)
    normed = (resid * lax.rsqrt(mean_sq + 1e-06) * norm_gain[...]).astype(BF16)

    for copy in (d1_copy, r1_copy, d2_copy, r2_copy):
        copy.wait()
    r_copy.start()
    decay_low = jnp.tanh(dot(normed, d1_buf[...])).astype(BF16)
    rate_low = dot(normed, r1_buf[...]).astype(BF16)
    pre = decay_base[...] + dot(decay_low, d2_buf[...])
    decay_out[...] = jnp.exp(-jnp.exp(-jax.nn.softplus(-pre) - 0.5))
    rate = jax.nn.sigmoid(rate_base[...] + dot(rate_low, r2_buf[...]))
    k_copy.wait()
    v_copy.start()
    keys_out[...] = dot(normed, wk_buf[...]).astype(BF16).astype(F32)
    r_copy.wait()
    state_copy(0).start()
    state_copy(1).start()
    recept = dot(normed, wr_buf[...]).astype(BF16).astype(F32)
    v_copy.wait()
    for g in range(2, groups):
        state_copy(g).start()
    all_rows = ids_t.shape[1]
    pick = (iota((all_rows, rows), 0) == iota((all_rows, rows), 1) + start[0]).astype(F32)
    own_ids = jnp.dot(ids_t[...].astype(F32), pick, preferred_element_type=F32)
    own_weights = jnp.dot(
        weights_t[...], pick, preferred_element_type=F32, precision=lax.Precision.HIGHEST
    )
    expert = iota((EXPERTS, rows), 0).astype(F32)
    hit0 = own_ids[0:1] == expert
    hit1 = own_ids[1:2] == expert
    member = jnp.where(hit0 | hit1, 1.0, 0.0)
    share = jnp.where(hit0, own_weights[0:1], 0.0) + jnp.where(hit1, own_weights[1:2], 0.0)
    before = (iota((rows, rows), 0) < iota((rows, rows), 1)).astype(F32)
    order = dot(member, before)
    spread = (iota((EXPERTS * ROWS, EXPERTS), 0) // ROWS == iota((EXPERTS * ROWS, EXPERTS), 1))
    spread = spread.astype(F32)
    member_r = dot(spread, member) > 0.5
    order_r = dot(spread, order).astype(jnp.int32)
    share_r = jnp.dot(spread, share, preferred_element_type=F32, precision=lax.Precision.HIGHEST)
    row = iota((EXPERTS * ROWS, rows), 0) % ROWS
    tables = [jnp.where(member_r & (row < CAP_DEV) & (order_r == row), 1.0, 0.0)]
    for j in range(SPLIT):
        slot = SPLIT * (row - CAP_DEV) + j
        tables.append(jnp.where(member_r & (row >= CAP_DEV) & (order_r == slot), 1.0, 0.0))
    for j in range(SPLIT + 1):
        combine[j] = (tables[j] * share_r).T

    vals_out[...] = dot(normed, wv_buf[...]).astype(BF16).astype(F32)

    for p in range(pairs):
        at = slice(p * 128, p * 128 + 128)
        k = keys_out[:, at]
        unit = k * lax.rsqrt(head_sums(k * k) + 1e-06)
        ua = unit * rate[:, at]
        r = recept[:, at]
        dr = decay_out[:, at] * r
        ua_out[:, at] = ua
        sums[0, :, at] = head_sums(ua * r)
        sums[1, :, at] = head_sums(k * r)
        for h in range(2):
            lanes = slice(h * 64, h * 64 + 64)
            lhs_buf[2 * p + h, 0:rows] = unit[:, lanes]
            lhs_buf[2 * p + h, rows : 2 * rows] = dr[:, lanes]

    own_block = iota((rows, 128), 1) // 64 == iota((rows, 128), 0) % 2
    low = iota((rows, 128), 1) < 64
    token = iota((rows, 128), 0) // 2

    def diagonal(x):
        total = jnp.zeros((rows, 128), F32)
        for c in range(rows * 64 // 128):
            total = total + jnp.where(own_block & (token == c), x[:, c * 128 : c * 128 + 128], 0.0)
        return total + pltpu.roll(total, 64, 1)

    def read_out(g):
        for p in range(g * step // 2, (g + 1) * step // 2):
            at = slice(p * 128, p * 128 + 128)
            found = []
            for head in (2 * p, 2 * p + 1):
                block = s_buf[:, head].reshape(rows * 64, 64).astype(BF16)
                found.append(
                    lax.dot_general(
                        lhs_buf[head].astype(BF16),
                        block,
                        (((1,), (1,)), ((), ())),
                        preferred_element_type=F32,
                    )
                )
            probe_out[:, at] = jnp.where(low, diagonal(found[0][:rows]), diagonal(found[1][:rows]))
            sums[2, :, at] = jnp.where(low, diagonal(found[0][rows:]), diagonal(found[1][rows:]))

    def normalized(p):
        at = slice(p * 128, p * 128 + 128)
        mixed = sums[2, :, at] - probe_out[:, at] * sums[0, :, at]
        mixed = mixed + vals_out[:, at] * sums[1, :, at]
        centre = mixed - head_sums(mixed) * (1.0 / 64)
        var = head_sums(centre * centre) * (1.0 / 64)
        return (centre * lax.rsqrt(var + 0.00064) * head_gain[:, at]).astype(BF16)

    pieces = []
    for g in range(groups):
        state_copy(g).wait()
        if g == 0:
            for copy in o_copies:
                copy.start()
        read_out(g)
        if g:
            pieces += [normalized(p) for p in range((g - 1) * step // 2, g * step // 2)]
    pieces += [normalized(p) for p in range((groups - 1) * step // 2, pairs)]
    mixed = jnp.concatenate(pieces, axis=1)
    total = resid
    for i in range(2):
        o_copies[i].wait()
        total = total + dot(mixed[:, i * half : i * half + half], wo_buf[pl.ds(i * half, half)])
    after[...] = total
    terms_copy = pltpu.make_async_copy(terms, terms_out, o_sem.at[0])
    terms_copy.start()

    mean_sq = jnp.mean(total * total, axis=1, keepdims=True)
    second = (total * lax.rsqrt(mean_sq + 1e-06) * second_gain[...]).astype(BF16)
    piece = width // (SPLIT + 1)
    last = second[:, SPLIT * piece :]
    copies = []
    for j in range(SPLIT):
        at = slice(j * piece, (j + 1) * piece)
        packed[:, at] = (
            dot(tables[0].astype(BF16), second[:, at]) + dot(tables[1 + j].astype(BF16), last)
        ).astype(BF16)
        at = pl.ds(j * piece, piece)
        copies.append(
            pltpu.make_async_copy(packed.at[:, at], packed_out.at[:, at], o_sem.at[1 + j])
        )
        copies[j].start()
    terms_copy.wait()
    for copy in copies:
        copy.wait()


def mixer(start, args, state, mats):
    rows, width = args[0].shape
    heads = state.shape[1]
    chan = heads * 64
    low = mats[3].shape[1]
    groups = 4
    f = lambda *s: jax.ShapeDtypeStruct(s, F32)
    v = pltpu.VMEM
    return pl.pallas_call(
        mixer_kernel,
        out_shape=(
            pltpu.HBM((EXPERTS * ROWS, width * SPLIT // (SPLIT + 1)), BF16),
            f(rows, width),
            f(SPLIT + 1, rows, EXPERTS * ROWS),
            pltpu.HBM((5, rows, chan), F32),
        ),
        in_specs=[SMEM] + [HBM] * (len(args) + 1 + len(mats)),
        out_specs=(HBM, VMEM, VMEM, HBM),
        scratch_shapes=[
            v((EXPERTS * ROWS, width * SPLIT // (SPLIT + 1)), BF16),
            v((5, rows, chan), F32),
            v(state.shape, F32),
            v((width, chan), BF16),
            v((width, chan), BF16),
            v((width, chan), BF16),
            v((width, low), BF16),
            v((low, chan), BF16),
            v((width, low), BF16),
            v((low, chan), BF16),
            v((chan, width), BF16),
            v((heads, 2 * rows, 64), F32),
            v((3, rows, chan), F32),
            *(v(a.shape, a.dtype) for a in args),
            pltpu.SemaphoreType.DMA((9,)),
            pltpu.SemaphoreType.DMA((groups,)),
            pltpu.SemaphoreType.DMA((len(args),)),
            pltpu.SemaphoreType.DMA((1 + SPLIT,)),
        ],
        compiler_params=pltpu.CompilerParams(vmem_limit_bytes=67_000_000),
        cost_estimate=pl.CostEstimate(
            flops=24_000_000_000, bytes_accessed=30_000_000, transcendentals=200_000
        ),
        name="mixer",
    )(start, *map(pin, (*args, state, *mats)))


def update_kernel(
    state,
    terms_in,
    out,
    buf,
    lhs,
    in_sem,
    out_sem,
    terms,
    t_sem,
):
    keys, vals, decay, ua, probe = (terms.at[i] for i in range(5))
    terms_copy = pltpu.make_async_copy(terms_in, terms, t_sem.at[0])
    terms_copy.start()
    rows, heads = buf.shape[0], buf.shape[1]
    pairs = heads // 2

    def load(p):
        at = pl.ds(p * 2, 2)
        return pltpu.make_async_copy(state.at[:, at], buf.at[:, at], in_sem.at[p])

    def store(p):
        at = pl.ds(p * 2, 2)
        return pltpu.make_async_copy(buf.at[:, at], out.at[:, at], out_sem.at[p])

    for p in range(pairs):
        load(p).start()

    column = iota((64, 4 * rows), 1) % rows
    terms_copy.wait()

    def body(p, carry):
        lanes = pl.ds(pl.multiple_of(p * 128, 128), 128)
        d = decay[:, lanes]
        u, q = ua[:, lanes], probe[:, lanes]
        u_high = u.astype(BF16).astype(F32)
        q_high = q.astype(BF16).astype(F32)
        left = jnp.concatenate([vals[:, lanes], q_high, q - q_high, q_high], axis=0).T
        right = jnp.concatenate([keys[:, lanes], -u_high, -u_high, u_high - u], axis=0)
        load(p).wait()
        for h in range(2):
            part = left[h * 64 : h * 64 + 64]
            for b in range(rows):
                lhs[h, b * 64 : b * 64 + 64] = jnp.where(column == b, part, 0.0).astype(BF16)
            if h:
                right = pltpu.roll(right, 64, 1)
                d = pltpu.roll(d, 64, 1)
            change = dot(lhs[h], right[:, :64].astype(BF16))
            for b in range(rows):
                buf[b, 2 * p + h] = (
                    buf[b, 2 * p + h] * d[b : b + 1, :64] + change[b * 64 : b * 64 + 64]
                )
        store(p).start()
        return carry

    lax.fori_loop(0, pairs, body, 0)
    for p in range(pairs):
        store(p).wait()


def update(state, terms):
    pairs = state.shape[1] // 2
    return pl.pallas_call(
        update_kernel,
        out_shape=jax.ShapeDtypeStruct(state.shape, F32),
        in_specs=[HBM] * 2,
        out_specs=HBM,
        scratch_shapes=[
            pltpu.VMEM(state.shape, F32),
            pltpu.VMEM((2, state.shape[0] * 64, 4 * state.shape[0]), BF16),
            pltpu.SemaphoreType.DMA((pairs,)),
            pltpu.SemaphoreType.DMA((pairs,)),
            pltpu.VMEM(terms.shape, F32),
            pltpu.SemaphoreType.DMA((1,)),
        ],
        compiler_params=pltpu.CompilerParams(vmem_limit_bytes=32 * 1024 * 1024),
        cost_estimate=pl.CostEstimate(
            flops=16_000_000_000, bytes_accessed=26_000_000, transcendentals=0
        ),
        name="update",
    )(pin(state), pin(terms))


def expert_kernel(chunk, group, *refs):
    received = refs[:group]
    gate, up, down = refs[group : group + 3]
    results = refs[group + 3 : 2 * group + 3]
    x_buf, acc = refs[2 * group + 3 :]
    width, hidden = gate.shape
    steps = hidden // chunk
    piece = width // (SPLIT + 1)
    slots = EXPERTS * CAP_DEV
    packed_rows = EXPERTS * ROWS

    source, c = iota((slots, packed_rows), 0) // CAP_DEV, iota((slots, packed_rows), 0) % CAP_DEV
    column = iota((slots, packed_rows), 1)
    tables = [jnp.where(column == source * ROWS + c, 1.0, 0.0).astype(BF16)]
    for j in range(SPLIT):
        here = (column == source * ROWS + CAP_DEV + c // SPLIT) & (c % SPLIT == j)
        tables.append(jnp.where(here, 1.0, 0.0).astype(BF16))
    for m in range(group):
        at = slice(m * slots, (m + 1) * slots)
        value = received[m][...]
        x_buf[at, : SPLIT * piece] = dot(tables[0], value).astype(BF16)
        x_buf[at, SPLIT * piece :] = sum(
            dot(tables[1 + j], value[:, j * piece : (j + 1) * piece]) for j in range(SPLIT)
        ).astype(BF16)

    for i in range(steps):
        at = slice(i * chunk, (i + 1) * chunk)
        x = x_buf[...]
        g = dot(x, gate[:, at])
        u = dot(x, up[:, at])
        h = (jax.nn.silu(g) * u).astype(BF16)
        y = dot(h, down[at])
        acc[...] = y if i == 0 else acc[...] + y

    for m in range(group):
        y = acc[m * slots : (m + 1) * slots].astype(BF16)
        last = y[:, SPLIT * piece :]
        for j in range(SPLIT):
            results[m][:, j * piece : (j + 1) * piece] = (
                dot_t(tables[0], y[:, j * piece : (j + 1) * piece]) + dot_t(tables[1 + j], last)
            ).astype(BF16)


def experts(received, gate, up, down):
    group = len(received)
    width, hidden = gate.shape
    chunk = next(c for c in (768, 384, 128) if hidden % c == 0)
    rows = group * EXPERTS * CAP_DEV
    return pl.pallas_call(
        functools.partial(expert_kernel, chunk, group),
        out_shape=tuple(jax.ShapeDtypeStruct(r.shape, BF16) for r in received),
        in_specs=[VMEM] * (group + 3),
        out_specs=(VMEM,) * group,
        scratch_shapes=[
            pltpu.VMEM((rows, width), BF16),
            pltpu.VMEM((rows, width), F32),
        ],
        compiler_params=pltpu.CompilerParams(vmem_limit_bytes=16 * 1024 * 1024),
        cost_estimate=pl.CostEstimate(
            flops=6 * rows * width * hidden, bytes_accessed=6 * width * hidden, transcendentals=0
        ),
        name="experts",
    )(*received, gate, up, down)


def window(value):
    return pl.pallas_call(
        lambda source, out: None,
        out_shape=jax.ShapeDtypeStruct(value.shape, value.dtype),
        in_specs=[HBM],
        out_specs=HBM,
        input_output_aliases={0: 0},
        compiler_params=pltpu.CompilerParams(vmem_limit_bytes=1024 * 1024),
        cost_estimate=pl.CostEstimate(
            flops=40_000_000_000, bytes_accessed=1024, transcendentals=0
        ),
        name="window",
    )(pin(value))


def combine_kernel(returned, after, combine, out):
    width = after.shape[1]
    piece = width // (SPLIT + 1)

    def blend(table, value):
        high = table.astype(BF16)
        low = (table - high.astype(F32)).astype(BF16)
        return dot(high, value) + dot(low, value)

    value = returned[...]
    first = blend(combine[0], value)
    last = sum(
        blend(combine[1 + j], value[:, j * piece : (j + 1) * piece]) for j in range(SPLIT)
    )
    at = SPLIT * piece
    out[:, :at] = (after[:, :at] + first).astype(BF16)
    out[:, at:] = (after[:, at:] + last).astype(BF16)


def on_device(
    tokens,
    state,
    norm_gain,
    w_recept,
    w_keys,
    w_values,
    decay_base,
    decay_first_matrix,
    decay_second_matrix,
    rate_base,
    rate_first_matrix,
    rate_second_matrix,
    head_gain,
    w_output,
    second_gain,
    route_ids,
    route_weights,
    expert_gate,
    expert_up,
    expert_down,
):
    devices = lax.axis_size("ep")
    group = devices // EXPERTS
    rows = tokens.shape[0]
    start = (lax.axis_index("ep") * rows).astype(jnp.int32).reshape(1)
    line = lambda a: a.reshape(1, -1)
    packed, after, combine, terms = mixer(
        start,
        (
            tokens,
            line(norm_gain),
            line(decay_base),
            line(rate_base),
            line(head_gain),
            line(second_gain),
            route_ids.T,
            route_weights.T,
        ),
        state,
        (
            w_recept,
            w_keys,
            w_values,
            decay_first_matrix,
            decay_second_matrix,
            rate_first_matrix,
            rate_second_matrix,
            w_output,
        ),
    )
    peers = [[e * group + j for e in range(EXPERTS)] for j in range(group)]
    cols = packed.shape[1]

    def exchange(value):
        chunks = value.reshape(EXPERTS, ROWS, cols)
        out = lax.all_to_all(
            chunks, "ep", split_axis=0, concat_axis=0, tiled=True, axis_index_groups=peers
        )
        return out.reshape(EXPERTS * ROWS, cols)

    def turn(value, by):
        return lax.ppermute(
            value,
            "ep",
            [(i, i // group * group + (i % group + by) % group) for i in range(devices)],
        )

    own = exchange(window(packed))
    new_state = update(state, terms)
    received = (own,) + tuple(turn(own, by) for by in range(1, group))
    results = experts(received, expert_gate, expert_up, expert_down)
    total = results[0].astype(F32)
    for by in range(1, group):
        total = total + turn(results[by], group - by).astype(F32)
    returned = exchange(total.astype(BF16))
    layer_out = pl.pallas_call(
        combine_kernel,
        out_shape=jax.ShapeDtypeStruct(after.shape, BF16),
        in_specs=[VMEM] * 3,
        out_specs=VMEM,
        compiler_params=pltpu.CompilerParams(vmem_limit_bytes=8 * 1024 * 1024),
        name="combine",
    )(returned, after, combine)
    return (layer_out, new_state)


def solution(mesh):
    in_specs = (
        P("ep", None),
        P("ep", None, None, None),
        P(),
        P(),
        P(),
        P(),
        P(),
        P(),
        P(),
        P(),
        P(),
        P(),
        P(),
        P(),
        P(),
        P(),
        P(),
        P(None, "ep"),
        P(None, "ep"),
        P("ep", None),
    )
    out_specs = (P("ep", None), P("ep", None, None, None))
    return jax.shard_map(
        on_device, mesh=mesh, in_specs=in_specs, out_specs=out_specs, check_vma=False
    )
```

```python
import functools

import jax
import jax.numpy as jnp
from jax import lax
from jax.experimental import pallas as pl
from jax.experimental.pallas import tpu as pltpu
from jax.sharding import PartitionSpec as P

EXPERTS = 16
CAP_DEV = 6
ROWS = 8
SPLIT = 3

F32 = jnp.float32
BF16 = jnp.bfloat16
HBM = pl.BlockSpec(memory_space=pltpu.HBM)
VMEM = pl.BlockSpec(memory_space=pltpu.VMEM)
SMEM = pl.BlockSpec(memory_space=pltpu.SMEM)


def pin(value):
    return pltpu.with_memory_space_constraint(value, pltpu.HBM)


def iota(shape, dim):
    return lax.broadcasted_iota(jnp.int32, shape, dim)


def dot(a, b):
    return jnp.dot(a, b, preferred_element_type=F32)


def head_sums(x):
    low = iota(x.shape, 1) < 64
    first = jnp.sum(jnp.where(low, x, 0.0), axis=1, keepdims=True)
    other = jnp.sum(jnp.where(low, 0.0, x), axis=1, keepdims=True)
    return jnp.where(low, first, other)


def mixer_kernel(
    start,
    tokens_in,
    norm_gain_in,
    decay_base_in,
    rate_base_in,
    head_gain_in,
    second_gain_in,
    ids_in,
    weights_in,
    state,
    w_recept,
    w_keys,
    w_values,
    decay_first,
    decay_second,
    rate_first,
    rate_second,
    w_output,
    packed_out,
    after,
    combine,
    terms_out,
    packed,
    terms,
    s_buf,
    wr_buf,
    wk_buf,
    wv_buf,
    d1_buf,
    d2_buf,
    r1_buf,
    r2_buf,
    wo_buf,
    lhs_buf,
    sums,
    tokens,
    norm_gain,
    decay_base,
    rate_base,
    head_gain,
    second_gain,
    ids_t,
    weights_t,
    w_sem,
    s_sem,
    a_sem,
    o_sem,
):
    keys_out, vals_out, decay_out, ua_out, probe_out = (terms.at[i] for i in range(5))
    rows, width = tokens.shape
    small = [
        pltpu.make_async_copy(src, dst, a_sem.at[i])
        for i, (src, dst) in enumerate(
            (
                (tokens_in, tokens),
                (norm_gain_in, norm_gain),
                (ids_in, ids_t),
                (weights_in, weights_t),
                (decay_base_in, decay_base),
                (rate_base_in, rate_base),
                (head_gain_in, head_gain),
                (second_gain_in, second_gain),
            )
        )
    ]
    for copy in small:
        copy.start()
    heads = state.shape[1]
    chan = heads * 64
    groups = s_sem.shape[0]
    step = heads // groups
    pairs = heads // 2

    def weight(i, src, dst):
        return pltpu.make_async_copy(src, dst, w_sem.at[i])

    def state_copy(g):
        return pltpu.make_async_copy(
            state.at[:, pl.ds(g * step, step)], s_buf.at[:, pl.ds(g * step, step)], s_sem.at[g]
        )

    k_copy = weight(0, w_keys, wk_buf)
    d1_copy = weight(1, decay_first, d1_buf)
    r1_copy = weight(2, rate_first, r1_buf)
    d2_copy = weight(3, decay_second, d2_buf)
    r2_copy = weight(4, rate_second, r2_buf)
    r_copy = weight(5, w_recept, wr_buf)
    v_copy = weight(6, w_values, wv_buf)
    half = chan // 2
    o_copies = [
        weight(7 + i, w_output.at[pl.ds(i * half, half)], wo_buf.at[pl.ds(i * half, half)])
        for i in range(2)
    ]
    for copy in (d1_copy, r1_copy, d2_copy, r2_copy, k_copy):
        copy.start()
    for copy in small:
        copy.wait()

    resid = tokens[...].astype(F32)
    mean_sq = jnp.mean(resid * resid, axis=1, keepdims=True)
    normed = (resid * lax.rsqrt(mean_sq + 1e-06) * norm_gain[...]).astype(BF16)

    for copy in (d1_copy, r1_copy, d2_copy, r2_copy):
        copy.wait()
    r_copy.start()
    decay_low = jnp.tanh(dot(normed, d1_buf[...])).astype(BF16)
    rate_low = dot(normed, r1_buf[...]).astype(BF16)
    pre = decay_base[...] + dot(decay_low, d2_buf[...])
    decay_out[...] = jnp.exp(-jnp.exp(-jax.nn.softplus(-pre) - 0.5))
    rate = jax.nn.sigmoid(rate_base[...] + dot(rate_low, r2_buf[...]))
    k_copy.wait()
    v_copy.start()
    keys_out[...] = dot(normed, wk_buf[...]).astype(BF16).astype(F32)
    r_copy.wait()
    state_copy(0).start()
    state_copy(1).start()
    recept = dot(normed, wr_buf[...]).astype(BF16).astype(F32)
    v_copy.wait()
    for g in range(2, groups):
        state_copy(g).start()
    all_rows = ids_t.shape[1]
    pick = (iota((all_rows, rows), 0) == iota((all_rows, rows), 1) + start[0]).astype(F32)
    own_ids = jnp.dot(ids_t[...].astype(F32), pick, preferred_element_type=F32)
    own_weights = jnp.dot(
        weights_t[...], pick, preferred_element_type=F32, precision=lax.Precision.HIGHEST
    )
    expert = iota((EXPERTS, rows), 0).astype(F32)
    hit0 = own_ids[0:1] == expert
    hit1 = own_ids[1:2] == expert
    member = jnp.where(hit0 | hit1, 1.0, 0.0)
    share = jnp.where(hit0, own_weights[0:1], 0.0) + jnp.where(hit1, own_weights[1:2], 0.0)
    before = (iota((rows, rows), 0) < iota((rows, rows), 1)).astype(F32)
    order = dot(member, before)
    spread = (iota((EXPERTS * ROWS, EXPERTS), 0) // ROWS == iota((EXPERTS * ROWS, EXPERTS), 1))
    spread = spread.astype(F32)
    member_r = dot(spread, member) > 0.5
    order_r = dot(spread, order).astype(jnp.int32)
    share_r = jnp.dot(spread, share, preferred_element_type=F32, precision=lax.Precision.HIGHEST)
    row = iota((EXPERTS * ROWS, rows), 0) % ROWS
    tables = [jnp.where(member_r & (row < CAP_DEV) & (order_r == row), 1.0, 0.0)]
    for j in range(SPLIT):
        slot = SPLIT * (row - CAP_DEV) + j
        tables.append(jnp.where(member_r & (row >= CAP_DEV) & (order_r == slot), 1.0, 0.0))
    for j in range(SPLIT + 1):
        combine[j] = (tables[j] * share_r).T

    vals_out[...] = dot(normed, wv_buf[...]).astype(BF16).astype(F32)

    for p in range(pairs):
        at = slice(p * 128, p * 128 + 128)
        k = keys_out[:, at]
        unit = k * lax.rsqrt(head_sums(k * k) + 1e-06)
        ua = unit * rate[:, at]
        r = recept[:, at]
        dr = decay_out[:, at] * r
        ua_out[:, at] = ua
        sums[0, :, at] = head_sums(ua * r)
        sums[1, :, at] = head_sums(k * r)
        for h in range(2):
            lanes = slice(h * 64, h * 64 + 64)
            lhs_buf[2 * p + h, 0:rows] = unit[:, lanes]
            lhs_buf[2 * p + h, rows : 2 * rows] = dr[:, lanes]

    own_block = iota((rows, 128), 1) // 64 == iota((rows, 128), 0) % 2
    low = iota((rows, 128), 1) < 64
    token = iota((rows, 128), 0) // 2

    def diagonal(x):
        total = jnp.zeros((rows, 128), F32)
        for c in range(rows * 64 // 128):
            total = total + jnp.where(own_block & (token == c), x[:, c * 128 : c * 128 + 128], 0.0)
        return total + pltpu.roll(total, 64, 1)

    def read_out(g):
        for p in range(g * step // 2, (g + 1) * step // 2):
            at = slice(p * 128, p * 128 + 128)
            found = []
            for head in (2 * p, 2 * p + 1):
                block = s_buf[:, head].reshape(rows * 64, 64).astype(BF16)
                found.append(
                    lax.dot_general(
                        lhs_buf[head].astype(BF16),
                        block,
                        (((1,), (1,)), ((), ())),
                        preferred_element_type=F32,
                    )
                )
            probe_out[:, at] = jnp.where(low, diagonal(found[0][:rows]), diagonal(found[1][:rows]))
            sums[2, :, at] = jnp.where(low, diagonal(found[0][rows:]), diagonal(found[1][rows:]))

    def normalized(p):
        at = slice(p * 128, p * 128 + 128)
        mixed = sums[2, :, at] - probe_out[:, at] * sums[0, :, at]
        mixed = mixed + vals_out[:, at] * sums[1, :, at]
        centre = mixed - head_sums(mixed) * (1.0 / 64)
        var = head_sums(centre * centre) * (1.0 / 64)
        return (centre * lax.rsqrt(var + 0.00064) * head_gain[:, at]).astype(BF16)

    pieces = []
    for g in range(groups):
        state_copy(g).wait()
        if g == 0:
            for copy in o_copies:
                copy.start()
        read_out(g)
        if g:
            pieces += [normalized(p) for p in range((g - 1) * step // 2, g * step // 2)]
    pieces += [normalized(p) for p in range((groups - 1) * step // 2, pairs)]
    mixed = jnp.concatenate(pieces, axis=1)
    total = resid
    for i in range(2):
        o_copies[i].wait()
        total = total + dot(mixed[:, i * half : i * half + half], wo_buf[pl.ds(i * half, half)])
    after[...] = total
    terms_copy = pltpu.make_async_copy(terms, terms_out, o_sem.at[0])
    terms_copy.start()

    mean_sq = jnp.mean(total * total, axis=1, keepdims=True)
    second = (total * lax.rsqrt(mean_sq + 1e-06) * second_gain[...]).astype(BF16)
    piece = width // (SPLIT + 1)
    last = second[:, SPLIT * piece :]
    copies = []
    for j in range(SPLIT):
        at = slice(j * piece, (j + 1) * piece)
        packed[:, at] = (
            dot(tables[0].astype(BF16), second[:, at]) + dot(tables[1 + j].astype(BF16), last)
        ).astype(BF16)
        at = pl.ds(j * piece, piece)
        copies.append(
            pltpu.make_async_copy(packed.at[:, at], packed_out.at[:, at], o_sem.at[1 + j])
        )
        copies[j].start()
    terms_copy.wait()
    for copy in copies:
        copy.wait()


def mixer(start, args, state, mats):
    rows, width = args[0].shape
    heads = state.shape[1]
    chan = heads * 64
    low = mats[3].shape[1]
    groups = 4
    f = lambda *s: jax.ShapeDtypeStruct(s, F32)
    v = pltpu.VMEM
    return pl.pallas_call(
        mixer_kernel,
        out_shape=(
            pltpu.HBM((EXPERTS * ROWS, width * SPLIT // (SPLIT + 1)), BF16),
            f(rows, width),
            f(SPLIT + 1, rows, EXPERTS * ROWS),
            pltpu.HBM((5, rows, chan), F32),
        ),
        in_specs=[SMEM] + [HBM] * (len(args) + 1 + len(mats)),
        out_specs=(HBM, VMEM, VMEM, HBM),
        scratch_shapes=[
            v((EXPERTS * ROWS, width * SPLIT // (SPLIT + 1)), BF16),
            v((5, rows, chan), F32),
            v(state.shape, F32),
            v((width, chan), BF16),
            v((width, chan), BF16),
            v((width, chan), BF16),
            v((width, low), BF16),
            v((low, chan), BF16),
            v((width, low), BF16),
            v((low, chan), BF16),
            v((chan, width), BF16),
            v((heads, 2 * rows, 64), F32),
            v((3, rows, chan), F32),
            *(v(a.shape, a.dtype) for a in args),
            pltpu.SemaphoreType.DMA((9,)),
            pltpu.SemaphoreType.DMA((groups,)),
            pltpu.SemaphoreType.DMA((len(args),)),
            pltpu.SemaphoreType.DMA((1 + SPLIT,)),
        ],
        compiler_params=pltpu.CompilerParams(vmem_limit_bytes=67_000_000),
        cost_estimate=pl.CostEstimate(
            flops=24_000_000_000, bytes_accessed=30_000_000, transcendentals=200_000
        ),
        name="mixer",
    )(start, *map(pin, (*args, state, *mats)))


def update_kernel(
    state,
    terms_in,
    out,
    buf,
    lhs,
    in_sem,
    out_sem,
    terms,
    t_sem,
):
    keys, vals, decay, ua, probe = (terms.at[i] for i in range(5))
    terms_copy = pltpu.make_async_copy(terms_in, terms, t_sem.at[0])
    terms_copy.start()
    rows, heads = buf.shape[0], buf.shape[1]
    pairs = heads // 2

    def load(p):
        at = pl.ds(p * 2, 2)
        return pltpu.make_async_copy(state.at[:, at], buf.at[:, at], in_sem.at[p])

    def store(p):
        at = pl.ds(p * 2, 2)
        return pltpu.make_async_copy(buf.at[:, at], out.at[:, at], out_sem.at[p])

    for p in range(pairs):
        load(p).start()

    column = iota((64, 4 * rows), 1) % rows
    terms_copy.wait()

    def body(p, carry):
        lanes = pl.ds(pl.multiple_of(p * 128, 128), 128)
        d = decay[:, lanes]
        u, q = ua[:, lanes], probe[:, lanes]
        u_high = u.astype(BF16).astype(F32)
        q_high = q.astype(BF16).astype(F32)
        left = jnp.concatenate([vals[:, lanes], q_high, q - q_high, q_high], axis=0).T
        right = jnp.concatenate([keys[:, lanes], -u_high, -u_high, u_high - u], axis=0)
        load(p).wait()
        for h in range(2):
            part = left[h * 64 : h * 64 + 64]
            for b in range(rows):
                lhs[h, b * 64 : b * 64 + 64] = jnp.where(column == b, part, 0.0).astype(BF16)
            if h:
                right = pltpu.roll(right, 64, 1)
                d = pltpu.roll(d, 64, 1)
            change = dot(lhs[h], right[:, :64].astype(BF16))
            for b in range(rows):
                buf[b, 2 * p + h] = (
                    buf[b, 2 * p + h] * d[b : b + 1, :64] + change[b * 64 : b * 64 + 64]
                )
        store(p).start()
        return carry

    lax.fori_loop(0, pairs, body, 0)
    for p in range(pairs):
        store(p).wait()


def update(state, terms):
    pairs = state.shape[1] // 2
    return pl.pallas_call(
        update_kernel,
        out_shape=jax.ShapeDtypeStruct(state.shape, F32),
        in_specs=[HBM] * 2,
        out_specs=HBM,
        scratch_shapes=[
            pltpu.VMEM(state.shape, F32),
            pltpu.VMEM((2, state.shape[0] * 64, 4 * state.shape[0]), BF16),
            pltpu.SemaphoreType.DMA((pairs,)),
            pltpu.SemaphoreType.DMA((pairs,)),
            pltpu.VMEM(terms.shape, F32),
            pltpu.SemaphoreType.DMA((1,)),
        ],
        compiler_params=pltpu.CompilerParams(vmem_limit_bytes=32 * 1024 * 1024),
        cost_estimate=pl.CostEstimate(
            flops=16_000_000_000, bytes_accessed=26_000_000, transcendentals=0
        ),
        name="update",
    )(pin(state), pin(terms))


def unpack_tables():
    shape = (EXPERTS * CAP_DEV, EXPERTS * ROWS)
    source, c, column = iota(shape, 0) // CAP_DEV, iota(shape, 0) % CAP_DEV, iota(shape, 1)
    tables = [jnp.where(column == source * ROWS + c, 1.0, 0.0).astype(BF16)]
    for j in range(SPLIT):
        here = (column == source * ROWS + CAP_DEV + c // SPLIT) & (c % SPLIT == j)
        tables.append(jnp.where(here, 1.0, 0.0).astype(BF16))
    return tables


def unpack(tables, value, out):
    piece = value.shape[1] // SPLIT
    out[:, : SPLIT * piece] = dot(tables[0], value).astype(BF16)
    out[:, SPLIT * piece :] = sum(
        dot(tables[1 + j], value[:, j * piece : (j + 1) * piece]) for j in range(SPLIT)
    ).astype(BF16)


def unpack_own(value):
    rows, width = EXPERTS * CAP_DEV, value.shape[1] * (SPLIT + 1) // SPLIT
    return pl.pallas_call(
        lambda source, out: unpack(unpack_tables(), source[...], out),
        out_shape=jax.ShapeDtypeStruct((rows, width), BF16),
        in_specs=[VMEM],
        out_specs=VMEM,
        compiler_params=pltpu.CompilerParams(vmem_limit_bytes=4 * 1024 * 1024),
        cost_estimate=pl.CostEstimate(
            flops=2_000_000_000, bytes_accessed=800_000, transcendentals=0
        ),
        name="unpack",
    )(value)


def expert_kernel(chunk, group, *refs):
    received = refs[:group]
    gate, up, down = refs[group : group + 3]
    results = refs[group + 3 : 2 * group + 3]
    x_buf, acc = refs[2 * group + 3 :]
    width, hidden = gate.shape
    steps = hidden // chunk
    piece = width // (SPLIT + 1)
    slots = EXPERTS * CAP_DEV
    packed_rows = EXPERTS * ROWS

    x_buf[:slots] = received[0][...]
    tables = unpack_tables()
    for m in range(1, group):
        at = slice(m * slots, (m + 1) * slots)
        unpack(tables, received[m][...], x_buf.at[at])

    for i in range(steps):
        at = slice(i * chunk, (i + 1) * chunk)
        x = x_buf[...]
        g = dot(x, gate[:, at])
        u = dot(x, up[:, at])
        h = (jax.nn.silu(g) * u).astype(BF16)
        y = dot(h, down[at])
        acc[...] = y if i == 0 else acc[...] + y

    source, c = iota((packed_rows, slots), 1) // CAP_DEV, iota((packed_rows, slots), 1) % CAP_DEV
    column = iota((packed_rows, slots), 0)
    tables = [jnp.where(column == source * ROWS + c, 1.0, 0.0).astype(BF16)]
    for j in range(SPLIT):
        here = (column == source * ROWS + CAP_DEV + c // SPLIT) & (c % SPLIT == j)
        tables.append(jnp.where(here, 1.0, 0.0).astype(BF16))
    for m in range(group):
        y = acc[m * slots : (m + 1) * slots].astype(BF16)
        last = y[:, SPLIT * piece :]
        for j in range(SPLIT):
            results[m][:, j * piece : (j + 1) * piece] = (
                dot(tables[0], y[:, j * piece : (j + 1) * piece]) + dot(tables[1 + j], last)
            ).astype(BF16)


def experts(own, received, gate, up, down):
    group = len(received)
    width, hidden = gate.shape
    chunk = next(c for c in (768, 384, 128) if hidden % c == 0)
    rows = group * EXPERTS * CAP_DEV
    return pl.pallas_call(
        functools.partial(expert_kernel, chunk, group),
        out_shape=tuple(jax.ShapeDtypeStruct(r.shape, BF16) for r in received),
        in_specs=[VMEM] * (group + 3),
        out_specs=(VMEM,) * group,
        scratch_shapes=[
            pltpu.VMEM((rows, width), BF16),
            pltpu.VMEM((rows, width), F32),
        ],
        compiler_params=pltpu.CompilerParams(vmem_limit_bytes=16 * 1024 * 1024),
        cost_estimate=pl.CostEstimate(
            flops=6 * rows * width * hidden, bytes_accessed=6 * width * hidden, transcendentals=0
        ),
        name="experts",
    )(own, *received[1:], gate, up, down)


def window(value):
    return pl.pallas_call(
        lambda source, out: None,
        out_shape=jax.ShapeDtypeStruct(value.shape, value.dtype),
        in_specs=[HBM],
        out_specs=HBM,
        input_output_aliases={0: 0},
        compiler_params=pltpu.CompilerParams(vmem_limit_bytes=1024 * 1024),
        cost_estimate=pl.CostEstimate(
            flops=40_000_000_000, bytes_accessed=1024, transcendentals=0
        ),
        name="window",
    )(pin(value))


def combine_kernel(returned, after, combine, out):
    width = after.shape[1]
    piece = width // (SPLIT + 1)

    def blend(table, value):
        high = table.astype(BF16)
        low = (table - high.astype(F32)).astype(BF16)
        return dot(high, value) + dot(low, value)

    value = returned[...]
    first = blend(combine[0], value)
    last = sum(
        blend(combine[1 + j], value[:, j * piece : (j + 1) * piece]) for j in range(SPLIT)
    )
    at = SPLIT * piece
    out[:, :at] = (after[:, :at] + first).astype(BF16)
    out[:, at:] = (after[:, at:] + last).astype(BF16)


def on_device(
    tokens,
    state,
    norm_gain,
    w_recept,
    w_keys,
    w_values,
    decay_base,
    decay_first_matrix,
    decay_second_matrix,
    rate_base,
    rate_first_matrix,
    rate_second_matrix,
    head_gain,
    w_output,
    second_gain,
    route_ids,
    route_weights,
    expert_gate,
    expert_up,
    expert_down,
):
    devices = lax.axis_size("ep")
    group = devices // EXPERTS
    rows = tokens.shape[0]
    start = (lax.axis_index("ep") * rows).astype(jnp.int32).reshape(1)
    line = lambda a: a.reshape(1, -1)
    packed, after, combine, terms = mixer(
        start,
        (
            tokens,
            line(norm_gain),
            line(decay_base),
            line(rate_base),
            line(head_gain),
            line(second_gain),
            route_ids.T,
            route_weights.T,
        ),
        state,
        (
            w_recept,
            w_keys,
            w_values,
            decay_first_matrix,
            decay_second_matrix,
            rate_first_matrix,
            rate_second_matrix,
            w_output,
        ),
    )
    peers = [[e * group + j for e in range(EXPERTS)] for j in range(group)]
    cols = packed.shape[1]

    def exchange(value):
        chunks = value.reshape(EXPERTS, ROWS, cols)
        out = lax.all_to_all(
            chunks, "ep", split_axis=0, concat_axis=0, tiled=True, axis_index_groups=peers
        )
        return out.reshape(EXPERTS * ROWS, cols)

    def turn(value, by):
        return lax.ppermute(
            value,
            "ep",
            [(i, i // group * group + (i % group + by) % group) for i in range(devices)],
        )

    own = exchange(window(packed))
    new_state = update(state, terms)
    received = (own,) + tuple(turn(own, by) for by in range(1, group))
    results = experts(unpack_own(own), received, expert_gate, expert_up, expert_down)
    total = results[0].astype(F32)
    for by in range(1, group):
        total = total + turn(results[by], group - by).astype(F32)
    returned = exchange(total.astype(BF16))
    layer_out = pl.pallas_call(
        combine_kernel,
        out_shape=jax.ShapeDtypeStruct(after.shape, BF16),
        in_specs=[VMEM] * 3,
        out_specs=VMEM,
        compiler_params=pltpu.CompilerParams(vmem_limit_bytes=8 * 1024 * 1024),
        name="combine",
    )(returned, after, combine)
    return (layer_out, new_state)


def solution(mesh):
    in_specs = (
        P("ep", None),
        P("ep", None, None, None),
        P(),
        P(),
        P(),
        P(),
        P(),
        P(),
        P(),
        P(),
        P(),
        P(),
        P(),
        P(),
        P(),
        P(),
        P(),
        P(None, "ep"),
        P(None, "ep"),
        P("ep", None),
    )
    out_specs = (P("ep", None), P("ep", None, None, None))
    return jax.shard_map(
        on_device, mesh=mesh, in_specs=in_specs, out_specs=out_specs, check_vma=False
    )
```
